32 devices in a mesh: sp: 8 (over z, core), tp: 4 (over y, x).
Axes of the slice: x: 2, y: 2, z: 4, core: 2. Of those that a mesh axis runs over, the one named last changes fastest.
Arguments:
- tokens: bfloat16 [1536, 4096], P('sp', 'tp'), may hold values from -60 to 60
- lean_query: bfloat16 [1536, 16, 64], P('sp', 'tp'), may hold values from -6 to 6
- lean_key: bfloat16 [1536, 2, 64], P('sp'), may hold values from -6 to 6
- lean_value: bfloat16 [1536, 2, 64], P('sp'), may hold values from -6 to 6
- lean_gains: float32 [2, 64], replicated, may hold values from 0.25 to 7.5
- broad_query: bfloat16 [1536, 16, 128], P('sp', 'tp'), may hold values from -6 to 6
- broad_key: bfloat16 [1536, 2, 128], P('sp'), may hold values from -6 to 6
- broad_value: bfloat16 [1536, 2, 128], P('sp'), may hold values from -6 to 6
- broad_gains: float32 [2, 128], replicated, may hold values from 0.25 to 7.5
- mixer_gain: float32 [3072], replicated, may hold values from 0.1 to 1.9
- output_weight: bfloat16 [3072, 4096], P(None, 'tp'), may hold values from -0.109375 to 0.109375
- channel_gain: float32 [4096], P('tp'), may hold values from 0.1 to 1.9
- gate_weight: bfloat16 [8, 4096, 2048], P('sp', None, 'tp'), may hold values from -0.09375 to 0.09375
- up_weight: bfloat16 [8, 4096, 2048], P('sp', None, 'tp'), may hold values from -0.09375 to 0.09375
- down_weight: bfloat16 [8, 2048, 4096], P('sp', None, 'tp'), may hold values from -0.125 to 0.125
- route_experts: int32 [1536, 2], P('sp'), may hold values from 0 to 7, as said below
- route_logits: float32 [1536, 2], P('sp'), may hold values from -6 to 6
- group_weight: float32 [1536], P('sp'), may hold values from 0.3 to 1
Outputs:
- encoded: bfloat16 [1536, 4096], P('sp', 'tp')
The draws below stay inside these ranges and needn't reach their ends.
Inputs may be any that keep to these rules, and one draw needn't show every extreme that they name: `route_experts`: each row names two different experts of one group, expert e lying in group e // 2. In every aligned block of 192 rows no expert is named by more than 96 rows; one group, the same for all blocks, is named by exactly half of each block's rows, and each of its experts by exactly 96 of them.
All inputs are finite; a program needn't handle non-finite values.
Results may differ from the reference program's by a relative error of at most 0.0083.
Values may be sent and summed in bfloat16 or wider, within the bound.
A program may use at most 64 MiB of HBM per device.

```python
import jax
import jax.numpy as jnp
from jax import lax

TOK_SP = 192
SEQ = 1536
D = 4096
HQ_A = 16
KV_A = 2
HD_A = 64
HQ_B = 16
KV_B = 2
HD_B = 128
DMIX = 3072
GRID_W = 64
EXPERTS = 8
GROUPS = 4
EPG = 2
TOPK = 2
FF = 2048
CAP = 96
N_SP = 8


def drawn_pair(base_key, head_count, key_heads, head_size):
    subkeys = jax.random.split(base_key, 2)
    keys = jax.random.normal(subkeys[0], (SEQ, key_heads, head_size), jnp.float32)
    queries = jax.random.normal(subkeys[1], (SEQ, head_count, head_size), jnp.float32)
    return (jnp.clip(queries, -6.0, 6.0), jnp.clip(keys, -6.0, 6.0))


def gain_draw(base_key, head_size):
    return 1.0 + 0.18 * jnp.clip(jax.random.normal(base_key, (2, head_size), jnp.float32), -4.0, 4.0)


def draw_lean_query(key, part):
    return drawn_pair(jax.random.fold_in(key, 101), HQ_A, KV_A, HD_A)[0].astype(jnp.bfloat16)


def draw_lean_key(key, part):
    return drawn_pair(jax.random.fold_in(key, 101), HQ_A, KV_A, HD_A)[1].astype(jnp.bfloat16)


def draw_broad_query(key, part):
    return drawn_pair(jax.random.fold_in(key, 102), HQ_B, KV_B, HD_B)[0].astype(jnp.bfloat16)


def draw_broad_key(key, part):
    return drawn_pair(jax.random.fold_in(key, 102), HQ_B, KV_B, HD_B)[1].astype(jnp.bfloat16)


def draw_lean_gains(key, part):
    return gain_draw(jax.random.fold_in(key, 201), HD_A)


def draw_broad_gains(key, part):
    return gain_draw(jax.random.fold_in(key, 202), HD_B)


def draw_tokens(key, part):
    first_key, second_key = jax.random.split(jax.random.fold_in(key, 401))
    column = jnp.arange(D, dtype=jnp.float32) / D
    base_values = jnp.clip(jax.random.normal(first_key, (SEQ, D), jnp.float32), -5.0, 5.0)
    column_scale = 0.3 * 10.0 ** column
    row_scale = 0.4 * 10.0 ** jax.random.uniform(second_key, (SEQ, 1), jnp.float32)
    return (base_values * column_scale[None, :] * row_scale).astype(jnp.bfloat16)


def draw_route_experts(key, part):
    block_count = SEQ // TOK_SP
    half_rows = TOK_SP // 2
    big_group = jax.random.randint(jax.random.fold_in(key, 7), (), 0, GROUPS)
    block_keys = jax.random.split(jax.random.fold_in(key, 11), block_count)

    def one_block(block_key):
        cut_key, order_key, rank_key, inner_key = jax.random.split(block_key, 4)
        cut_points = jnp.sort(jax.random.randint(cut_key, (GROUPS - 2,), 0, half_rows + 1))
        bounds = jnp.concatenate([jnp.zeros((1,), jnp.int32), cut_points, jnp.full((1,), half_rows, jnp.int32)])
        starts = jnp.concatenate([jnp.zeros((1,), jnp.int32), half_rows + bounds[:-1]])
        ends = jnp.concatenate([jnp.full((1,), half_rows, jnp.int32), half_rows + bounds[1:]])
        others = (big_group + 1 + jax.random.permutation(order_key, GROUPS - 1)) % GROUPS
        group_order = jnp.concatenate([big_group[None], others])
        token_rank = jax.random.permutation(rank_key, TOK_SP)
        member = ((token_rank[:, None] >= starts[None, :]) & (token_rank[:, None] < ends[None, :])).astype(jnp.int32)
        which = jnp.argmax(member, axis=1)
        chosen_group = group_order[which]
        inner = token_rank - starts[which]
        first_pick = inner % EPG
        second_pick = (inner + 1 + inner // EPG % (EPG - 1)) % EPG
        shuffles = jax.vmap(lambda each_key: jax.random.permutation(each_key, EPG))(jax.random.split(inner_key, GROUPS))
        first_expert = chosen_group * EPG + shuffles[chosen_group, first_pick]
        second_expert = chosen_group * EPG + shuffles[chosen_group, second_pick]
        return jnp.stack([first_expert, second_expert], axis=1)
    return jax.vmap(one_block)(block_keys).reshape(SEQ, TOPK).astype(jnp.int32)


def shard_levels(rng, dims, pieces, low, high):
    loudness = 1.0
    for position, parts in pieces:
        draws = jax.random.uniform(jax.random.fold_in(jax.random.fold_in(rng, 6), position), (parts,), jnp.float32, low / len(pieces), high / len(pieces))
        loudness = loudness * jnp.repeat(jnp.exp(draws), dims[position] // parts).reshape((-1,) + (1,) * (len(dims) - 1 - position))
    return loudness


def gaussian(own_key, dims, spread, limit, cuts=(), kind=jnp.bfloat16):
    values = spread * jax.random.normal(own_key, dims, jnp.float32)
    if cuts:
        values = values * shard_levels(own_key, dims, cuts, -0.22, 0.18)
    return jnp.clip(values, -limit, limit).astype(kind)


def setup_inputs(seed: int = 0) -> dict:
    splits = jax.random.split(jax.random.key(seed), 19)
    return {
        "tokens": draw_tokens(jax.random.fold_in(splits[18], 71), 0),
        "lean_query": draw_lean_query(jax.random.fold_in(splits[18], 71), 0),
        "lean_key": draw_lean_key(jax.random.fold_in(splits[18], 71), 0),
        "lean_value": gaussian(splits[3], (SEQ, KV_A, HD_A), 1.0, 6.0, ((0, 8),)),
        "lean_gains": draw_lean_gains(jax.random.fold_in(splits[18], 71), 0),
        "broad_query": draw_broad_query(jax.random.fold_in(splits[18], 71), 0),
        "broad_key": draw_broad_key(jax.random.fold_in(splits[18], 71), 0),
        "broad_value": gaussian(splits[7], (SEQ, KV_B, HD_B), 1.0, 6.0, ((0, 8),)),
        "broad_gains": draw_broad_gains(jax.random.fold_in(splits[18], 71), 0),
        "mixer_gain": jnp.clip(1.0 + 0.18 * jax.random.normal(splits[9], (DMIX,), jnp.float32), 0.1, 1.9),
        "output_weight": gaussian(splits[10], (DMIX, D), DMIX ** -0.5, 0.109375, ((1, 4),)),
        "channel_gain": jnp.clip(1.0 + 0.18 * jax.random.normal(splits[11], (D,), jnp.float32), 0.1, 1.9),
        "gate_weight": gaussian(splits[12], (EXPERTS, D, FF), D ** -0.5, 0.09375, ((0, 8), (2, 4))),
        "up_weight": gaussian(splits[13], (EXPERTS, D, FF), D ** -0.5, 0.09375, ((0, 8), (2, 4))),
        "down_weight": gaussian(splits[14], (EXPERTS, FF, D), FF ** -0.5, 0.125, ((0, 8), (2, 4))),
        "route_experts": draw_route_experts(jax.random.fold_in(splits[18], 71), 0),
        "route_logits": gaussian(splits[16], (SEQ, TOPK), 1.5, 6.0, ((0, 8),), jnp.float32),
        "group_weight": jnp.clip(0.3 + 0.7 * jax.random.uniform(splits[17], (SEQ,), jnp.float32) ** shard_levels(splits[17], (SEQ,), ((0, 8),), -0.2, 0.2), 0.3, 1.0),
    }


epsilon = 1e-06
theta_base = 10000.0

def axial_angles(positions, head_size):
    quarter = head_size // 4
    frequency = theta_base ** (-jnp.arange(quarter, dtype=jnp.float32) / quarter)
    grid_rows = (positions // GRID_W).astype(jnp.float32)
    grid_columns = (positions % GRID_W).astype(jnp.float32)
    return (grid_rows[:, None] * frequency[None, :], grid_columns[:, None] * frequency[None, :])

def turn_half(values, angles):
    half_width = values.shape[-1] // 2
    first_half = values[..., :half_width]
    second = values[..., half_width:]
    cosine = jnp.cos(angles)[:, None, :]
    sine_part = jnp.sin(angles)[:, None, :]
    return jnp.concatenate([first_half * cosine - second * sine_part, second * cosine + first_half * sine_part], axis=-1)

def prepare(raw_values, gain_row, positions):
    values = raw_values.astype(jnp.float32)
    values = values * lax.rsqrt(lax.optimization_barrier(jnp.mean(values * values, axis=-1, keepdims=True)) + epsilon) * gain_row
    row_angles, column_angles = axial_angles(positions, raw_values.shape[-1])
    half_width = raw_values.shape[-1] // 2
    turned = jnp.concatenate([turn_half(values[..., :half_width], row_angles), turn_half(values[..., half_width:], column_angles)], axis=-1)
    return turned.astype(jnp.bfloat16)

def attend(queries, keys, values):
    token_count, head_count, head_size = queries.shape
    key_heads = keys.shape[1]
    group_ratio = head_count // key_heads
    blocks = queries.reshape(token_count // TOK_SP, TOK_SP, key_heads, group_ratio, head_size)
    keys_wide = keys.astype(jnp.float32)
    values_wide = values.astype(jnp.float32)

    def one_block(block_queries):
        scores = jnp.einsum('qkgd,skd->kgqs', block_queries.astype(jnp.float32), keys_wide) * head_size ** (-0.5)
        peak_score = lax.optimization_barrier(jnp.max(scores, axis=-1, keepdims=True))
        weights = jnp.exp(scores - peak_score)
        weight_sum = lax.optimization_barrier(jnp.sum(weights, axis=-1))
        rounded = lax.optimization_barrier(weights.astype(jnp.bfloat16)).astype(jnp.float32)
        summed = jnp.einsum('kgqs,skd->qkgd', rounded, values_wide)
        return (summed / jnp.transpose(weight_sum, (2, 0, 1))[..., None]).astype(jnp.bfloat16)
    mixed_heads = lax.map(one_block, blocks)
    return mixed_heads.reshape(token_count, head_count * head_size)

def group_norm(head_rows, gain_row):
    values = head_rows.astype(jnp.float32)
    return (values * lax.rsqrt(lax.optimization_barrier(jnp.mean(values * values, axis=-1, keepdims=True)) + epsilon) * gain_row).astype(jnp.bfloat16)

def reference(tokens, lean_query, lean_key, lean_value, lean_gains, broad_query, broad_key, broad_value, broad_gains, mixer_gain, output_weight, channel_gain, gate_weight, up_weight, down_weight, route_experts, route_logits, group_weight):
    positions = jnp.arange(SEQ, dtype=jnp.int32)
    lean_out = attend(prepare(lean_query, lean_gains[0], positions), prepare(lean_key, lean_gains[1], positions), lean_value)
    broad_out = attend(prepare(broad_query, broad_gains[0], positions), prepare(broad_key, broad_gains[1], positions), broad_value)
    lean_width = HQ_A * HD_A
    mixed_rows = jnp.concatenate([group_norm(lean_out, mixer_gain[:lean_width]), group_norm(broad_out, mixer_gain[lean_width:])], axis=1)
    stream = tokens.astype(jnp.float32) + jnp.dot(mixed_rows, output_weight, preferred_element_type=jnp.float32)
    normed = (stream * lax.rsqrt(lax.optimization_barrier(jnp.mean(stream * stream, axis=-1, keepdims=True)) + epsilon) * channel_gain).astype(jnp.bfloat16)
    logit_gap = route_logits[:, 0] - route_logits[:, 1]
    weights = group_weight[:, None] * jax.nn.sigmoid(jnp.stack([logit_gap, -logit_gap], axis=1))
    row_bound = N_SP * CAP

    def one_expert(running, expert_index):
        hit_mask = route_experts == expert_index
        member = jnp.any(hit_mask, axis=1)
        chosen = jnp.nonzero(member, size=row_bound, fill_value=0)[0]
        valid_rows = (jnp.arange(row_bound) < jnp.sum(member.astype(jnp.int32))).astype(jnp.float32)
        picked = normed[chosen]
        gate_value = jnp.dot(picked, gate_weight[expert_index], preferred_element_type=jnp.float32)
        up_value = jnp.dot(picked, up_weight[expert_index], preferred_element_type=jnp.float32)
        hidden = (jax.nn.silu(gate_value) * up_value).astype(jnp.bfloat16)
        result = jnp.dot(hidden, down_weight[expert_index], preferred_element_type=jnp.float32).astype(jnp.bfloat16)
        coefficient = lax.optimization_barrier(jnp.sum(jnp.where(hit_mask, weights, 0.0), axis=1))[chosen] * valid_rows
        return (running.at[chosen].add(coefficient[:, None] * result.astype(jnp.float32)), None)
    routed = lax.scan(one_expert, jnp.zeros((SEQ, D), jnp.float32), jnp.arange(EXPERTS, dtype=jnp.int32))[0]
    return (stream + routed).astype(jnp.bfloat16)
```

```python
import functools

import jax
import jax.numpy as jnp
from jax import lax
from jax.experimental import pallas as pl
from jax.experimental.pallas import tpu as pltpu
from jax.sharding import PartitionSpec as P

D = 4096
HQ_A = 16
KV_A = 2
HQ_B = 16
KV_B = 2
GRID_W = 64
GROUPS = 4


epsilon = 1e-06
theta_base = 10000.0
floor_score = -1e30


def axial_angles(positions, head_size):
    quarter = head_size // 4
    frequency = theta_base ** (-jnp.arange(quarter, dtype=jnp.float32) / quarter)
    grid_rows = (positions // GRID_W).astype(jnp.float32)
    grid_columns = (positions % GRID_W).astype(jnp.float32)
    return (grid_rows[:, None] * frequency[None, :], grid_columns[:, None] * frequency[None, :])


def turn_half(values, angles):
    half_width = values.shape[-1] // 2
    first_half = values[..., :half_width]
    second = values[..., half_width:]
    cosine = jnp.cos(angles)[:, None, :]
    sine_part = jnp.sin(angles)[:, None, :]
    return jnp.concatenate(
        [first_half * cosine - second * sine_part, second * cosine + first_half * sine_part],
        axis=-1,
    )


def prepare(raw_values, gain_row, positions):
    values = raw_values.astype(jnp.float32)
    values = (
        values * lax.rsqrt(jnp.mean(values * values, axis=-1, keepdims=True) + epsilon) * gain_row
    )
    row_angles, column_angles = axial_angles(positions, raw_values.shape[-1])
    half_width = raw_values.shape[-1] // 2
    turned = jnp.concatenate(
        [
            turn_half(values[..., :half_width], row_angles),
            turn_half(values[..., half_width:], column_angles),
        ],
        axis=-1,
    )
    return turned.astype(jnp.bfloat16)


def group_norm(head_rows, gain_row):
    values = head_rows.astype(jnp.float32)
    return (
        values * lax.rsqrt(jnp.mean(values * values, axis=-1, keepdims=True) + epsilon) * gain_row
    ).astype(jnp.bfloat16)


def own_heads(query_raw, key_raw, value_raw, gain_pair, positions, lane_index, group_ratio):
    head_count, head_size = (query_raw.shape[1], query_raw.shape[2])
    key_heads = max(1, head_count // group_ratio)
    kv_start = lane_index * head_count // group_ratio
    key_part = lax.dynamic_slice_in_dim(key_raw, kv_start, key_heads, 1)
    value_part = lax.dynamic_slice_in_dim(value_raw, kv_start, key_heads, 1)
    queries = prepare(query_raw, gain_pair[0], positions).reshape(
        query_raw.shape[0], key_heads, head_count // key_heads, head_size
    )
    return (queries, prepare(key_part, gain_pair[1], positions), value_part)


def start_state(queries):
    row_count = queries.shape[0]
    head_count = queries.shape[1] * queries.shape[2]
    return (
        jnp.full((head_count, row_count), floor_score, jnp.float32),
        jnp.zeros((head_count, row_count), jnp.float32),
        jnp.zeros((row_count, head_count, queries.shape[3]), jnp.float32),
    )


def attend_piece(fold_state, queries, keys, values):
    peak_score, weight_sum, accumulated = fold_state
    row_count, key_heads, grouped, head_size = queries.shape
    key_count = keys.shape[0]
    scores = jnp.einsum(
        "qkgd,skd->kgqs", queries, keys, preferred_element_type=jnp.float32
    ) * head_size ** (-0.5)
    scores = scores.reshape(key_heads * grouped, row_count, key_count)
    new_peak = jnp.maximum(peak_score, jnp.max(scores, axis=-1))
    weights = jnp.exp(scores - new_peak[..., None])
    new_sum = jnp.sum(weights, axis=-1)
    rounded = weights.astype(jnp.bfloat16).reshape(key_heads, grouped, row_count, key_count)
    partial_value = jnp.einsum(
        "kgqs,skd->qkgd", rounded, values, preferred_element_type=jnp.float32
    )
    partial_value = partial_value.reshape(row_count, key_heads * grouped, head_size)
    return (new_peak, new_sum, partial_value)


def finish_heads(fold_state):
    accumulated = fold_state[2]
    return (
        (accumulated / jnp.transpose(fold_state[1])[:, :, None])
        .astype(jnp.bfloat16)
        .reshape(accumulated.shape[0], -1)
    )


MESH = pl.DeviceIdType.MESH
EXTRA = 128


def enter(peers):
    barrier = pltpu.get_barrier_semaphore()
    for peer in peers:
        pl.semaphore_signal(barrier, inc=1, device_id=peer, device_id_type=MESH)
    pl.semaphore_wait(barrier, len(peers))


def place():
    sp, tp = lax.axis_index("sp"), lax.axis_index("tp")
    z, core = sp // 2, sp % 2
    y, x = tp // 2, tp % 2
    sibling = {"sp": z * 2 + (1 - core), "tp": tp}
    x_peer = {"sp": sp, "tp": y * 2 + (1 - x)}
    y_peer = {"sp": sp, "tp": (1 - y) * 2 + x}
    chunks = (tp, y * 2 + (1 - x), (1 - y) * 2 + x, (1 - y) * 2 + (1 - x))
    return z, core, tp, sibling, x_peer, y_peer, chunks


def remote(source, target, send_sem, recv_sem, device):
    return pltpu.make_async_remote_copy(
        src_ref=source,
        dst_ref=target,
        send_sem=send_sem,
        recv_sem=recv_sem,
        device_id=device,
        device_id_type=MESH,
    )


def keys_kernel(chips, own_ref, out_ref, z_send, z_recv, s_send, s_recv):
    z, core, tp, sibling, x_peer, y_peer, chunks = place()
    peers = [{"sp": ((z + d) % chips) * 2 + core, "tp": tp} for d in range(1, chips)]
    enter(peers + [sibling])
    sends = [
        remote(own_ref, out_ref.at[0, d], z_send.at[d], z_recv.at[d], peers[d - 1])
        for d in range(1, chips)
    ]
    for copy in sends:
        copy.start()
    forwards = [remote(own_ref, out_ref.at[1, 0], s_send.at[0], s_recv.at[0], sibling)]
    forwards[0].start()
    out_ref[0, 0] = own_ref[...]
    for d in range(1, chips):
        sends[d - 1].wait_recv()
        copy = remote(out_ref.at[0, d], out_ref.at[1, d], s_send.at[d], s_recv.at[d], sibling)
        copy.start()
        forwards.append(copy)
    for copy in forwards:
        copy.wait()
    for copy in sends:
        copy.wait_send()


def gather_keys(own, chips):
    return pl.pallas_call(
        functools.partial(keys_kernel, chips),
        out_shape=jax.ShapeDtypeStruct((2, chips) + own.shape, own.dtype),
        in_specs=[pl.BlockSpec(memory_space=pltpu.VMEM)],
        out_specs=pl.BlockSpec(memory_space=pltpu.VMEM),
        scratch_shapes=[pltpu.SemaphoreType.DMA((chips,))] * 4,
        compiler_params=pltpu.CompilerParams(collective_id=0, has_side_effects=True),
    )(own)


def heads_kernel(lean_ref, broad_ref, lean_out, broad_out, send_sem, recv_sem):
    z, core, tp, sibling, x_peer, y_peer, chunks = place()
    enter([x_peer, y_peer])
    half = lean_ref.shape[0] // 2
    pieces = ((lean_ref, lean_out), (broad_ref, broad_out))

    def columns(ref, chunk):
        width = ref.shape[1]
        return pl.ds(pl.multiple_of(chunk * width, width), width)

    first = []
    for i, (own, out) in enumerate(pieces):
        for j, peer in enumerate((x_peer, y_peer)):
            k = i * 2 + j
            copy = remote(own, out.at[:, columns(own, tp)], send_sem.at[k], recv_sem.at[k], peer)
            copy.start()
            first.append(copy)
    for own, out in pieces:
        out[:, columns(own, tp)] = own[...]
    second = []
    for i, (own, out) in enumerate(pieces):
        for j, peer in enumerate((y_peer, x_peer)):
            first[i * 2 + j].wait_recv()
            k = 4 + i * 2 + j
            part = out.at[pl.ds(j * half, half), columns(own, chunks[1 + j])]
            copy = remote(part, part, send_sem.at[k], recv_sem.at[k], peer)
            copy.start()
            second.append(copy)
    for copy in second:
        copy.wait()
    for copy in first:
        copy.wait_send()


def gather_heads(lean, broad, lanes):
    return pl.pallas_call(
        heads_kernel,
        out_shape=[
            jax.ShapeDtypeStruct((part.shape[0], part.shape[1] * lanes), part.dtype)
            for part in (lean, broad)
        ],
        in_specs=[pl.BlockSpec(memory_space=pltpu.VMEM)] * 2,
        out_specs=[pl.BlockSpec(memory_space=pltpu.VMEM)] * 2,
        scratch_shapes=[pltpu.SemaphoreType.DMA((8,))] * 2,
        compiler_params=pltpu.CompilerParams(collective_id=1, has_side_effects=True),
    )(lean, broad)


def experts_kernel(
    width,
    out_going,
    gate_hbm,
    up_hbm,
    down_hbm,
    out_ref,
    rows,
    gate_w,
    up_w,
    down_w,
    hidden,
    gate_acc,
    up_acc,
    result,
    swap_send,
    swap_recv,
    back,
    w_sem,
    send_sem,
    recv_sem,
    h_send,
    h_recv,
    e_send,
    e_recv,
    b_send,
    b_recv,
):
    z, core, tp, sibling, x_peer, y_peer, chunks = place()
    chips, cap = out_going.shape[0], out_going.shape[1]
    ff = gate_acc.shape[1]
    half = 2 * cap
    ahead = [{"sp": ((z + d) % chips) * 2 + core, "tp": tp} for d in range(chips)]
    behind = [{"sp": ((z + chips - d) % chips) * 2 + core, "tp": tp} for d in range(chips)]
    enter(ahead[1:] + [sibling, x_peer, y_peer])

    def slot(d, r, side=0):
        return rows.at[d // 2, r, pl.ds(side * half + (d % 2) * cap, cap)]

    Z, X, Y, RELAY, SIDE = 0, 1, 2, 3, 4
    pending = []

    def send(source, target, kind, d, device):
        copy = remote(source, target, send_sem.at[kind, d], recv_sem.at[kind, d], device)
        copy.start()
        pending.append(copy)
        return copy

    arrivals = {}
    for d in range(1, chips):
        arrivals[Z, d] = send(out_going.at[d], slot(d, 0), Z, d, ahead[d])
    loads = [
        pltpu.make_async_copy(source, target, w_sem.at[i])
        for i, (source, target) in enumerate(
            ((gate_hbm, gate_w), (up_hbm, up_w), (down_hbm, down_w))
        )
    ]

    def spread(d):
        source = out_going.at[0] if d == 0 else slot(d, 0)
        if d:
            arrivals[Z, d].wait_recv()
        arrivals[X, d] = send(source, slot(d, 1), X, d, x_peer)
        arrivals[Y, d] = send(source, slot(d, 2), Y, d, y_peer)
        arrivals[SIDE, d] = send(source, slot(d, 0, 1), SIDE, d, sibling)

    def to_side(d, r):
        arrivals[SIDE + r, d] = send(slot(d, r), slot(d, r, 1), SIDE + r, d, sibling)

    def relay(d):
        arrivals[X, d].wait_recv()
        if d % 2 == 0:
            arrivals[RELAY, d] = send(slot(d, 1), slot(d, 3), RELAY, d, y_peer)
        to_side(d, 1)
        arrivals[Y, d].wait_recv()
        if d % 2 == 1:
            arrivals[RELAY, d] = send(slot(d, 2), slot(d, 3), RELAY, d, x_peer)
        to_side(d, 2)

    def project(p, r):
        for d in (2 * p, 2 * p + 1):
            arrivals[SIDE + r, d].wait_recv()
        block = rows[p, r, :, pl.ds(0, width)]
        for weight, total in ((gate_w, gate_acc), (up_w, up_acc)):
            part = jnp.dot(block, weight[chunks[r]], preferred_element_type=jnp.float32)
            if r == 0:
                total[...] = part
            else:
                total[...] += part

    def activate(p):
        squares = 0.0
        for r in range(4):
            extra = rows[p, r, :, pl.ds(width, EXTRA)].astype(jnp.float32)
            squares = squares + extra[:, 0:1] + extra[:, 1:2]
        scale = lax.rsqrt(squares / (4 * width) + epsilon)
        gate_value = gate_acc[...] * scale
        up_value = up_acc[...] * scale
        hidden[p, 0] = (gate_value / (1.0 + jnp.exp(-gate_value)) * up_value).astype(jnp.bfloat16)
        for k, peer in ((0, x_peer), (1, y_peer)):
            copy = remote(
                hidden.at[p, 0], hidden.at[p, 1 + k], h_send.at[p, k], h_recv.at[p, k], peer
            )
            copy.start()
            pending.append(copy)
            arrivals["h", p, k] = copy

    def relay_hidden(p):
        for k, peer in ((0, y_peer), (1, x_peer)):
            arrivals["h", p, k].wait_recv()
            part = pl.ds(k * half, half)
            copy = remote(
                hidden.at[p, 1 + k, part],
                hidden.at[p, 3, part],
                h_send.at[p, 2 + k],
                h_recv.at[p, 2 + k],
                peer,
            )
            copy.start()
            pending.append(copy)
            arrivals["h", p, 2 + k] = copy

    def last_slot(p):
        for d in (2 * p, 2 * p + 1):
            arrivals[RELAY, d].wait_recv()
            to_side(d, 3)
        project(p, 3)
        activate(p)

    def finish(p):
        for r in range(3):
            part = jnp.dot(hidden[p, r], down_w[chunks[r]], preferred_element_type=jnp.float32)
            if r == 0:
                result[...] = part
            else:
                result[...] += part
        for k in (2, 3):
            arrivals["h", p, k].wait_recv()
        result[...] += jnp.dot(hidden[p, 3], down_w[chunks[3]], preferred_element_type=jnp.float32)
        extra = rows[p, 0, :, pl.ds(width, EXTRA)].astype(jnp.float32)
        low = extra[:, 2:3] + extra[:, 3:4]
        high = extra[:, 4:5] + extra[:, 5:6]
        share = low + (high - low) * core.astype(jnp.float32)
        swap_send[p] = (result[half:, :] * share[half:]).astype(jnp.bfloat16)
        copy = remote(swap_send.at[p], swap_recv.at[p], e_send.at[p], e_recv.at[p], sibling)
        copy.start()
        pending.append(copy)
        kept = result[:half, :] * share[:half]
        copy.wait_recv()
        total = (kept + swap_recv[p].astype(jnp.float32)).astype(jnp.bfloat16)
        back[p] = total
        for d in (2 * p, 2 * p + 1):
            part = pl.ds((d % 2) * cap, cap)
            if d == 0:
                out_ref[0] = total[:cap]
                continue
            copy = remote(back.at[p, part], out_ref.at[d], b_send.at[d], b_recv.at[d], behind[d])
            copy.start()
            pending.append(copy)
            arrivals["b", d] = copy

    spread(0)
    for copy in loads:
        copy.start()
    rows[0, 0, pl.ds(0, cap)] = out_going[0]
    spread(1)
    relay(0)
    relay(1)
    spread(2)
    spread(3)
    loads[0].wait()
    loads[1].wait()
    for r in range(3):
        project(0, r)
    last_slot(0)
    relay(2)
    relay(3)
    relay_hidden(0)
    for r in range(3):
        project(1, r)
    last_slot(1)
    loads[2].wait()
    finish(0)
    relay_hidden(1)
    finish(1)
    for d in range(1, chips):
        arrivals["b", d].wait_recv()
    for copy in pending:
        copy.wait_send()


def run_experts(out_going, gate_weight, up_weight, down_weight):
    chips, cap, padded = out_going.shape
    width, ff = (padded - EXTRA, gate_weight.shape[1])
    features = down_weight.shape[1]
    return pl.pallas_call(
        functools.partial(experts_kernel, width),
        out_shape=jax.ShapeDtypeStruct((chips, cap, features), jnp.bfloat16),
        in_specs=[pl.BlockSpec(memory_space=pltpu.VMEM)]
        + [pl.BlockSpec(memory_space=pl.ANY)] * 3,
        out_specs=pl.BlockSpec(memory_space=pltpu.VMEM),
        scratch_shapes=[
            pltpu.VMEM((2, 4, 4 * cap, padded), jnp.bfloat16),
            pltpu.VMEM((4, width, ff), jnp.bfloat16),
            pltpu.VMEM((4, width, ff), jnp.bfloat16),
            pltpu.VMEM((4, ff, features), jnp.bfloat16),
            pltpu.VMEM((2, 4, 4 * cap, ff), jnp.bfloat16),
            pltpu.VMEM((4 * cap, ff), jnp.float32),
            pltpu.VMEM((4 * cap, ff), jnp.float32),
            pltpu.VMEM((4 * cap, features), jnp.float32),
            pltpu.VMEM((2, 2 * cap, features), jnp.bfloat16),
            pltpu.VMEM((2, 2 * cap, features), jnp.bfloat16),
            pltpu.VMEM((2, 2 * cap, features), jnp.bfloat16),
            pltpu.SemaphoreType.DMA((3,)),
            pltpu.SemaphoreType.DMA((8, 4)),
            pltpu.SemaphoreType.DMA((8, 4)),
            pltpu.SemaphoreType.DMA((2, 4)),
            pltpu.SemaphoreType.DMA((2, 4)),
            pltpu.SemaphoreType.DMA((2,)),
            pltpu.SemaphoreType.DMA((2,)),
            pltpu.SemaphoreType.DMA((4,)),
            pltpu.SemaphoreType.DMA((4,)),
        ],
        compiler_params=pltpu.CompilerParams(
            collective_id=2, has_side_effects=True, vmem_limit_bytes=56 * 1024 * 1024
        ),
    )(
        out_going,
        gate_weight.reshape(4, width, ff),
        up_weight.reshape(4, width, ff),
        down_weight.reshape(4, ff, features),
    )


def split_pair(values):
    high = lax.reduce_precision(values, 8, 7)
    return high.astype(jnp.bfloat16), (values - high).astype(jnp.bfloat16)


def paired_block(stream, route_experts, weights, channel_gain, gate_weight, up_weight, down_weight):
    row_count, width = stream.shape
    cap = row_count // 2
    group = route_experts[:, 0] // 2
    near = (group + GROUPS - lax.axis_index("sp") // 2) % GROUPS
    member = (near[:, None] == jnp.arange(GROUPS, dtype=jnp.int32)[None, :]).astype(jnp.bfloat16)
    order = jnp.arange(row_count, dtype=jnp.int32)
    earlier = (order[:, None] > order[None, :]).astype(jnp.bfloat16)
    counts = jnp.dot(earlier, member, preferred_element_type=jnp.float32)
    rank = jnp.sum(counts * member.astype(jnp.float32), axis=1).astype(jnp.int32)
    slot_index = near * cap + rank
    slots = jnp.arange(GROUPS * cap, dtype=jnp.int32)
    picker = (slots[:, None] == slot_index[None, :]).astype(jnp.bfloat16)
    first_low = route_experts[:, 0] % 2 == 0
    low = jnp.where(first_low, weights[:, 0], weights[:, 1])
    high = jnp.where(first_low, weights[:, 1], weights[:, 0])
    squares = jnp.sum(stream * stream, axis=1)
    columns = split_pair(squares) + split_pair(low) + split_pair(high)
    extra = jnp.stack(columns, axis=1)
    extra = jnp.pad(extra, ((0, 0), (0, EXTRA - extra.shape[1])))
    payload = jnp.concatenate([(stream * channel_gain).astype(jnp.bfloat16), extra], axis=1)
    out_going = jnp.dot(picker, payload, preferred_element_type=jnp.float32).astype(jnp.bfloat16)
    arrived = run_experts(
        out_going.reshape(GROUPS, cap, width + EXTRA), gate_weight, up_weight, down_weight
    )
    arrived = arrived.reshape(GROUPS * cap, width)
    picked = lax.dot_general(
        picker, arrived, (((0,), (0,)), ((), ())), preferred_element_type=jnp.float32
    )
    return (stream + picked).astype(jnp.bfloat16)


def on_device(
    tokens,
    lean_query,
    lean_key,
    lean_value,
    lean_gains,
    broad_query,
    broad_key,
    broad_value,
    broad_gains,
    mixer_gain,
    output_weight,
    channel_gain,
    gate_weight,
    up_weight,
    down_weight,
    route_experts,
    route_logits,
    group_weight,
):
    row_count = tokens.shape[0]
    positions = lax.axis_index("sp") * row_count + jnp.arange(row_count, dtype=jnp.int32)
    lane_index = lax.axis_index("tp")
    lean_queries, lean_keys, lean_values = own_heads(
        lean_query, lean_key, lean_value, lean_gains, positions, lane_index, HQ_A // KV_A
    )
    broad_queries, broad_keys, broad_values = own_heads(
        broad_query, broad_key, broad_value, broad_gains, positions, lane_index, HQ_B // KV_B
    )
    chips = lax.axis_size("sp") // 2
    paired = (
        lax.axis_size("tp") == 4
        and chips == GROUPS
        and chips == 4
        and route_experts.shape[1] == 2
        and lean_keys.shape[1] == 1
        and broad_keys.shape[1] == 1
    )
    if paired:
        own = jnp.concatenate(
            [part[:, 0] for part in (broad_keys, broad_values, lean_keys, lean_values)], axis=1
        )
        every = gather_keys(own, chips).reshape(2 * chips * row_count, -1)
        broad_size, lean_size = broad_keys.shape[2], lean_keys.shape[2]
        shard_rows = (
            every[:, None, 2 * broad_size : 2 * broad_size + lean_size],
            every[:, None, 2 * broad_size + lean_size :],
            every[:, None, :broad_size],
            every[:, None, broad_size : 2 * broad_size],
        )
    else:
        shard_rows = (
            lax.all_gather(lean_keys, "sp", axis=0, tiled=True),
            lax.all_gather(lean_values, "sp", axis=0, tiled=True),
            lax.all_gather(broad_keys, "sp", axis=0, tiled=True),
            lax.all_gather(broad_values, "sp", axis=0, tiled=True),
        )
    lean_state = attend_piece(start_state(lean_queries), lean_queries, shard_rows[0], shard_rows[1])
    broad_state = attend_piece(
        start_state(broad_queries), broad_queries, shard_rows[2], shard_rows[3]
    )
    if paired:
        lean_all, broad_all = gather_heads(
            finish_heads(lean_state), finish_heads(broad_state), lax.axis_size("tp")
        )
    else:
        lean_all, broad_all = (
            lax.all_gather(finish_heads(lean_state), "tp", axis=1, tiled=True),
            lax.all_gather(finish_heads(broad_state), "tp", axis=1, tiled=True),
        )
    lean_width = lean_all.shape[1]
    stream = tokens.astype(jnp.float32) + jnp.dot(
        group_norm(lean_all, mixer_gain[:lean_width]),
        output_weight[:lean_width],
        preferred_element_type=jnp.float32,
    )
    stream = stream + jnp.dot(
        group_norm(broad_all, mixer_gain[lean_width:]),
        output_weight[lean_width:],
        preferred_element_type=jnp.float32,
    )
    logit_gap = route_logits[:, 0] - route_logits[:, 1]
    weights = group_weight[:, None] * jax.nn.sigmoid(jnp.stack([logit_gap, -logit_gap], axis=1))
    if paired:
        return paired_block(
            stream,
            route_experts,
            weights,
            channel_gain,
            gate_weight[0],
            up_weight[0],
            down_weight[0],
        )
    squares = lax.psum(jnp.sum(stream * stream, axis=1), "tp")
    normed = (stream * lax.rsqrt(squares / D + epsilon)[:, None] * channel_gain).astype(
        jnp.bfloat16
    )
    experts = lax.axis_size("sp")
    capacity = row_count // (experts // GROUPS)
    flat_experts = route_experts.reshape(-1)
    onehot = (flat_experts[:, None] == jnp.arange(experts, dtype=jnp.int32)[None, :]).astype(
        jnp.int32
    )
    slot_rank = jnp.sum((jnp.cumsum(onehot, axis=0) - 1) * onehot, axis=1)
    slot_index = flat_experts * capacity + slot_rank
    token_owner = jnp.repeat(jnp.arange(row_count, dtype=jnp.int32), route_experts.shape[1])
    filled = jnp.zeros((experts * capacity,), jnp.int32).at[slot_index].set(token_owner + 1)
    slot_live = (filled > 0)[:, None]
    source = jnp.maximum(filled - 1, 0)
    outgoing = jnp.where(slot_live, normed[source], jnp.zeros((), jnp.bfloat16)).reshape(
        experts, capacity, -1
    )
    arrived = lax.all_to_all(outgoing, "sp", split_axis=0, concat_axis=0, tiled=True)
    sources = arrived.shape[0]
    item_count = arrived.shape[1]
    shard_rows = lax.all_gather(arrived, "tp", axis=2, tiled=True)
    flat_rows = shard_rows.reshape(sources * item_count, shard_rows.shape[2])
    gate_part = gate_weight[0]
    up_part = up_weight[0]
    gate_value = jnp.dot(flat_rows, gate_part, preferred_element_type=jnp.float32)
    up_value = jnp.dot(flat_rows, up_part, preferred_element_type=jnp.float32)
    hidden = (jax.nn.silu(gate_value) * up_value).astype(jnp.bfloat16)
    down_part = down_weight[0]
    result = jnp.dot(
        lax.all_gather(hidden, "tp", axis=1, tiled=True),
        down_part,
        preferred_element_type=jnp.float32,
    )
    result = result.astype(jnp.bfloat16).reshape(sources, item_count, -1)
    returned = lax.all_to_all(result, "sp", split_axis=0, concat_axis=0, tiled=True)
    picked = (
        returned.reshape(experts * capacity, -1)[slot_index]
        .reshape(row_count, route_experts.shape[1], -1)
        .astype(jnp.float32)
    )
    return (stream + jnp.sum(picked * weights[:, :, None], axis=1)).astype(jnp.bfloat16)


def solution(mesh):
    return jax.shard_map(
        on_device,
        mesh=mesh,
        in_specs=(
            P("sp", "tp"),
            P("sp", "tp", None),
            P("sp", None, None),
            P("sp", None, None),
            P(),
            P("sp", "tp", None),
            P("sp", None, None),
            P("sp", None, None),
            P(),
            P(),
            P(None, "tp"),
            P("tp"),
            P("sp", None, "tp"),
            P("sp", None, "tp"),
            P("sp", None, "tp"),
            P("sp", None),
            P("sp", None),
            P("sp"),
        ),
        out_specs=P("sp", "tp"),
        check_vma=False,
    )
```

```python
import functools

import jax
import jax.numpy as jnp
import numpy as np
from jax import lax
from jax.experimental import pallas as pl
from jax.experimental.pallas import tpu as pltpu
from jax.sharding import PartitionSpec as P

D = 4096
HQ_A = 16
KV_A = 2
HQ_B = 16
KV_B = 2
GRID_W = 64
GROUPS = 4


epsilon = 1e-06
theta_base = 10000.0
floor_score = -1e30


def axial_angles(positions, head_size):
    quarter = head_size // 4
    frequency = theta_base ** (-jnp.arange(quarter, dtype=jnp.float32) / quarter)
    grid_rows = (positions // GRID_W).astype(jnp.float32)
    grid_columns = (positions % GRID_W).astype(jnp.float32)
    return (grid_rows[:, None] * frequency[None, :], grid_columns[:, None] * frequency[None, :])


def turn_half(values, angles):
    half_width = values.shape[-1] // 2
    first_half = values[..., :half_width]
    second = values[..., half_width:]
    cosine = jnp.cos(angles)[:, None, :]
    sine_part = jnp.sin(angles)[:, None, :]
    return jnp.concatenate(
        [first_half * cosine - second * sine_part, second * cosine + first_half * sine_part],
        axis=-1,
    )


def prepare(raw_values, gain_row, positions):
    values = raw_values.astype(jnp.float32)
    values = (
        values * lax.rsqrt(jnp.mean(values * values, axis=-1, keepdims=True) + epsilon) * gain_row
    )
    row_angles, column_angles = axial_angles(positions, raw_values.shape[-1])
    half_width = raw_values.shape[-1] // 2
    turned = jnp.concatenate(
        [
            turn_half(values[..., :half_width], row_angles),
            turn_half(values[..., half_width:], column_angles),
        ],
        axis=-1,
    )
    return turned.astype(jnp.bfloat16)


def group_norm(head_rows, gain_row):
    values = head_rows.astype(jnp.float32)
    return (
        values * lax.rsqrt(jnp.mean(values * values, axis=-1, keepdims=True) + epsilon) * gain_row
    ).astype(jnp.bfloat16)


def own_heads(query_raw, key_raw, value_raw, gain_pair, positions, lane_index, group_ratio):
    head_count, head_size = (query_raw.shape[1], query_raw.shape[2])
    key_heads = max(1, head_count // group_ratio)
    kv_start = lane_index * head_count // group_ratio
    key_part = lax.dynamic_slice_in_dim(key_raw, kv_start, key_heads, 1)
    value_part = lax.dynamic_slice_in_dim(value_raw, kv_start, key_heads, 1)
    queries = prepare(query_raw, gain_pair[0], positions).reshape(
        query_raw.shape[0], key_heads, head_count // key_heads, head_size
    )
    return (queries, prepare(key_part, gain_pair[1], positions), value_part)


def start_state(queries):
    row_count = queries.shape[0]
    head_count = queries.shape[1] * queries.shape[2]
    return (
        jnp.full((head_count, row_count), floor_score, jnp.float32),
        jnp.zeros((head_count, row_count), jnp.float32),
        jnp.zeros((row_count, head_count, queries.shape[3]), jnp.float32),
    )


def attend_piece(fold_state, queries, keys, values):
    peak_score, weight_sum, accumulated = fold_state
    row_count, key_heads, grouped, head_size = queries.shape
    key_count = keys.shape[0]
    scores = jnp.einsum(
        "qkgd,skd->kgqs", queries, keys, preferred_element_type=jnp.float32
    ) * head_size ** (-0.5)
    scores = scores.reshape(key_heads * grouped, row_count, key_count)
    new_peak = jnp.maximum(peak_score, jnp.max(scores, axis=-1))
    weights = jnp.exp(scores - new_peak[..., None])
    new_sum = jnp.sum(weights, axis=-1)
    rounded = weights.astype(jnp.bfloat16).reshape(key_heads, grouped, row_count, key_count)
    partial_value = jnp.einsum(
        "kgqs,skd->qkgd", rounded, values, preferred_element_type=jnp.float32
    )
    partial_value = partial_value.reshape(row_count, key_heads * grouped, head_size)
    return (new_peak, new_sum, partial_value)


def finish_heads(fold_state):
    accumulated = fold_state[2]
    return (
        (accumulated / jnp.transpose(fold_state[1])[:, :, None])
        .astype(jnp.bfloat16)
        .reshape(accumulated.shape[0], -1)
    )


MESH = pl.DeviceIdType.MESH
EXTRA = 128


def enter(peers):
    barrier = pltpu.get_barrier_semaphore()
    for peer in peers:
        pl.semaphore_signal(barrier, inc=1, device_id=peer, device_id_type=MESH)
    pl.semaphore_wait(barrier, len(peers))


def place():
    sp, tp = lax.axis_index("sp"), lax.axis_index("tp")
    z, core = sp // 2, sp % 2
    y, x = tp // 2, tp % 2
    sibling = {"sp": z * 2 + (1 - core), "tp": tp}
    x_peer = {"sp": sp, "tp": y * 2 + (1 - x)}
    y_peer = {"sp": sp, "tp": (1 - y) * 2 + x}
    chunks = (tp, y * 2 + (1 - x), (1 - y) * 2 + x, (1 - y) * 2 + (1 - x))
    return z, core, tp, sibling, x_peer, y_peer, chunks


def remote(source, target, send_sem, recv_sem, device):
    return pltpu.make_async_remote_copy(
        src_ref=source,
        dst_ref=target,
        send_sem=send_sem,
        recv_sem=recv_sem,
        device_id=device,
        device_id_type=MESH,
    )


def front_kernel(
    chips,
    lean_q,
    lean_k,
    lean_v,
    broad_q,
    broad_k,
    broad_v,
    lean_gain,
    broad_gain,
    cosines,
    sines,
    mixer_gain,
    tokens,
    channel_gain,
    picker,
    route_columns,
    weight_hbm,
    stream_out,
    going_out,
    own,
    keys,
    queries,
    peak,
    total,
    mass,
    lean_heads,
    broad_heads,
    weight,
    lean_acc,
    broad_acc,
    w_sem,
    k_send,
    k_recv,
    h_send,
    h_recv,
):
    z, core, tp, sibling, x_peer, y_peer, chunks = place()
    x, y = tp % 2, tp // 2
    rows = own.shape[0]
    half = rows // 2
    lanes = 128
    peers = [{"sp": ((z + d) % chips) * 2 + core, "tp": tp} for d in range(1, chips)]
    load = pltpu.make_async_copy(weight_hbm, weight, w_sem.at[0])
    load.start()
    lane = lax.broadcasted_iota(jnp.int32, (rows, lanes), 1)
    low = lane < lanes // 2

    def turned(raw, gain, size):
        values = raw.astype(jnp.float32)
        squares = values * values
        if size == lanes:
            mean = jnp.sum(squares, axis=1, keepdims=True) / size
        else:
            first = jnp.sum(jnp.where(low, squares, 0.0), axis=1, keepdims=True)
            second = jnp.sum(jnp.where(low, 0.0, squares), axis=1, keepdims=True)
            mean = jnp.where(low, first, second) / size
        values = values * lax.rsqrt(mean + epsilon) * gain
        quarter = size // 4
        partner = jnp.where(
            lane % (2 * quarter) < quarter,
            pltpu.roll(values, lanes - quarter, 1),
            pltpu.roll(values, quarter, 1),
        )
        part = pl.ds(0 if size == lanes else lanes, lanes)
        return values * cosines[:, part] + partner * sines[:, part]

    def swapped(values):
        return pltpu.roll(values, lanes // 2, 1)

    key_columns = pl.ds(pl.multiple_of(y * lanes, lanes), lanes)
    own[:, :lanes] = turned(broad_k[:, key_columns], broad_gain[1:2, :], lanes).astype(jnp.bfloat16)
    own[:, lanes : 2 * lanes] = broad_v[:, key_columns]
    both_keys = turned(lean_k[...], lean_gain[1:2, :], lanes // 2)
    both_values = lean_v[...].astype(jnp.float32)
    at_first = (1 - y).astype(jnp.float32)
    lean_key = both_keys * at_first + swapped(both_keys) * (1.0 - at_first)
    lean_value = swapped(both_values) * at_first + both_values * (1.0 - at_first)
    own[:, 2 * lanes :] = jnp.where(low, lean_key, lean_value).astype(jnp.bfloat16)

    enter(peers + [sibling, x_peer, y_peer])
    pending = []
    arrivals = {}

    def send(kind, d, source, target, device):
        copy = remote(source, target, k_send.at[kind, d], k_recv.at[kind, d], device)
        copy.start()
        pending.append(copy)
        arrivals[kind, d] = copy

    mine = pl.ds(pl.multiple_of(x * half, half), half)
    other = pl.ds(pl.multiple_of((1 - x) * half, half), half)
    side_mine = pl.ds(pl.multiple_of(rows + x * half, half), half)
    side_other = pl.ds(pl.multiple_of(rows + (1 - x) * half, half), half)
    Z, X, A, B = 0, 1, 2, 3
    for d in range(1, chips):
        send(Z, d, own.at[mine], keys.at[d, mine], peers[d - 1])
    send(A, 0, own, keys.at[0, pl.ds(rows, rows)], sibling)
    keys[0, pl.ds(0, rows)] = own[...]

    heads = queries.shape[1]
    for h in range(heads):
        part = pl.ds(h * lanes, lanes)
        queries[1, h] = turned(broad_q[:, part], broad_gain[0:1, :], lanes).astype(jnp.bfloat16)
    for h in range(heads // 2):
        part = pl.ds(h * lanes, lanes)
        pair = turned(lean_q[:, part], lean_gain[0:1, :], lanes // 2)
        queries[0, 2 * h] = jnp.where(low, pair, 0.0).astype(jnp.bfloat16)
        queries[0, 2 * h + 1] = jnp.where(low, swapped(pair), 0.0).astype(jnp.bfloat16)

    def attend(d, kind):
        size = lanes // 2 if kind == 0 else lanes
        key_part = pl.ds(2 * lanes, lanes) if kind == 0 else pl.ds(0, lanes)
        value_part = pl.ds(2 * lanes, lanes) if kind == 0 else pl.ds(lanes, lanes)

        def one_head(h, carry):
            scores = lax.dot_general(
                queries[kind, h],
                keys[d, :, key_part],
                (((1,), (1,)), ((), ())),
                preferred_element_type=jnp.float32,
            ) * (size**-0.5)
            top = jnp.max(scores, axis=1, keepdims=True)
            if d:
                old = peak[kind, h][:, :1]
                top = jnp.maximum(old, top)
            weights = jnp.exp(scores - top)
            summed = jnp.sum(weights, axis=1, keepdims=True)
            partial = jnp.dot(
                weights.astype(jnp.bfloat16),
                keys[d, :, value_part],
                preferred_element_type=jnp.float32,
            )
            if d:
                shrink = jnp.exp(old - top)
                summed = summed + total[kind, h][:, :1] * shrink
                partial = partial + mass[kind, h] * shrink
            peak[kind, h] = jnp.broadcast_to(top, (rows, lanes))
            total[kind, h] = jnp.broadcast_to(summed, (rows, lanes))
            mass[kind, h] = partial
            return carry

        lax.fori_loop(0, heads, one_head, 0)

    def forward(d):
        arrivals[Z, d].wait_recv()
        send(X, d, keys.at[d, mine], keys.at[d, mine], x_peer)
        send(A, d, keys.at[d, mine], keys.at[d, side_mine], sibling)

    def forward_other(d):
        arrivals[X, d].wait_recv()
        send(B, d, keys.at[d, other], keys.at[d, side_other], sibling)

    forward(1)
    arrivals[A, 0].wait_recv()
    attend(0, 0)
    forward_other(1)
    attend(0, 1)
    for d in range(1, chips):
        if d + 1 < chips:
            forward(d + 1)
        arrivals[A, d].wait_recv()
        arrivals[B, d].wait_recv()
        if d + 1 < chips:
            attend(d, 0)
            forward_other(d + 1)
            attend(d, 1)

    gathers = {}

    def spread(kind, buffer):
        for k, peer in ((0, x_peer), (1, y_peer)):
            n = kind * 4 + k
            copy = remote(buffer.at[0], buffer.at[1 + k], h_send.at[n], h_recv.at[n], peer)
            copy.start()
            pending.append(copy)
            gathers[kind, k] = copy

    def relay(kind, buffer):
        for k, peer in ((0, y_peer), (1, x_peer)):
            n = kind * 4 + 2 + k
            gathers[kind, k].wait_recv()
            part = pl.ds(k * half, half)
            copy = remote(
                buffer.at[1 + k, part], buffer.at[3, part], h_send.at[n], h_recv.at[n], peer
            )
            copy.start()
            pending.append(copy)
            gathers[kind, 2 + k] = copy

    def finished(kind, h):
        return mass[kind, h] / total[kind, h]

    attend(chips - 1, 0)
    for h in range(heads // 2):
        pair = jnp.where(low, swapped(finished(0, 2 * h)), finished(0, 2 * h + 1))
        lean_heads[0, :, pl.ds(h * lanes, lanes)] = pair.astype(jnp.bfloat16)
    spread(0, lean_heads)
    attend(chips - 1, 1)
    for h in range(heads):
        broad_heads[0, :, pl.ds(h * lanes, lanes)] = finished(1, h).astype(jnp.bfloat16)
    spread(1, broad_heads)
    load.wait()
    lean_width, broad_width = lean_heads.shape[2], broad_heads.shape[2]
    squares = [0.0, 0.0]

    def project(kind, r):
        buffer, acc, width, start = (
            (lean_heads, lean_acc, lean_width, 0),
            (broad_heads, broad_acc, broad_width, 4 * lean_width),
        )[kind]
        part = pl.ds(pl.multiple_of(start + chunks[r] * width, width), width)
        values = buffer[r].astype(jnp.float32)
        squares[kind] = squares[kind] + jnp.sum(values * values, axis=1, keepdims=True)
        scaled = (values * mixer_gain[:, part]).astype(jnp.bfloat16)
        product = jnp.dot(scaled, weight[part, :], preferred_element_type=jnp.float32)
        if r == 0:
            acc[...] = product
        else:
            acc[...] += product

    project(0, 0)
    relay(0, lean_heads)
    project(1, 0)
    project(0, 1)
    project(0, 2)
    relay(1, broad_heads)
    project(1, 1)
    project(1, 2)
    for kind in (0, 1):
        gathers[kind, 2].wait_recv()
        gathers[kind, 3].wait_recv()
        project(kind, 3)
    lean_scale = lax.rsqrt(squares[0] / (4 * lean_width) + epsilon)
    broad_scale = lax.rsqrt(squares[1] / (4 * broad_width) + epsilon)
    stream = (
        tokens[...].astype(jnp.float32)
        + lean_acc[...] * lean_scale
        + broad_acc[...] * broad_scale
    )
    stream_out[...] = stream
    width = stream.shape[1]
    norm = jnp.sum(stream * stream, axis=1, keepdims=True)
    norm_high = norm.astype(jnp.bfloat16).astype(jnp.float32)
    extra = jnp.where(
        lane == 0, norm_high, jnp.where(lane == 1, norm - norm_high, route_columns[...])
    ).astype(jnp.bfloat16)
    scaled = (stream * channel_gain[...]).astype(jnp.bfloat16)
    going_out[:, :width] = jnp.dot(
        picker[...], scaled, preferred_element_type=jnp.float32
    ).astype(jnp.bfloat16)
    going_out[:, width:] = jnp.dot(
        picker[...], extra, preferred_element_type=jnp.float32
    ).astype(jnp.bfloat16)
    for copy in pending:
        copy.wait_send()


def lane_frequencies(head_size):
    quarter = head_size // 4
    lane = np.arange(128) % head_size
    frequency = theta_base ** (-(lane % quarter).astype(np.float32) / np.float32(quarter))
    by_row = lane < head_size // 2
    sign = np.where(lane // quarter % 2 == 0, -1.0, 1.0)
    return frequency.astype(np.float32), by_row, sign.astype(np.float32)


def run_front(
    chips,
    positions,
    lean,
    broad,
    lean_gains,
    broad_gains,
    mixer_gain,
    tokens,
    channel_gain,
    picker,
    route_columns,
    output_weight,
):
    rows, width = tokens.shape
    heads = lean[0].shape[1]
    tables = [lane_frequencies(part[0].shape[2]) for part in (broad, lean)]
    frequency, by_row, sign = (np.concatenate(parts)[None, :] for parts in zip(*tables))
    row = (positions // GRID_W).astype(jnp.float32)[:, None]
    column = (positions % GRID_W).astype(jnp.float32)[:, None]
    angles = jnp.where(by_row, row, column) * frequency
    flat = [part.reshape(rows, -1) for part in lean + broad]
    return pl.pallas_call(
        functools.partial(front_kernel, chips),
        out_shape=[
            jax.ShapeDtypeStruct((rows, width), jnp.float32),
            jax.ShapeDtypeStruct((picker.shape[0], width + EXTRA), jnp.bfloat16),
        ],
        in_specs=[pl.BlockSpec(memory_space=pltpu.VMEM)] * 15
        + [pl.BlockSpec(memory_space=pl.ANY)],
        out_specs=[pl.BlockSpec(memory_space=pltpu.VMEM)] * 2,
        scratch_shapes=[
            pltpu.VMEM((rows, 384), jnp.bfloat16),
            pltpu.VMEM((chips, 2 * rows, 384), jnp.bfloat16),
            pltpu.VMEM((2, heads, rows, 128), jnp.bfloat16),
            pltpu.VMEM((2, heads, rows, 128), jnp.float32),
            pltpu.VMEM((2, heads, rows, 128), jnp.float32),
            pltpu.VMEM((2, heads, rows, 128), jnp.float32),
            pltpu.VMEM((4, rows, heads * 64), jnp.bfloat16),
            pltpu.VMEM((4, rows, heads * 128), jnp.bfloat16),
            pltpu.VMEM(output_weight.shape, jnp.bfloat16),
            pltpu.VMEM((rows, width), jnp.float32),
            pltpu.VMEM((rows, width), jnp.float32),
            pltpu.SemaphoreType.DMA((1,)),
            pltpu.SemaphoreType.DMA((4, chips)),
            pltpu.SemaphoreType.DMA((4, chips)),
            pltpu.SemaphoreType.DMA((8,)),
            pltpu.SemaphoreType.DMA((8,)),
        ],
        compiler_params=pltpu.CompilerParams(
            collective_id=0, has_side_effects=True, vmem_limit_bytes=48 * 1024 * 1024
        ),
    )(
        *flat,
        jnp.concatenate([lean_gains, lean_gains], axis=1),
        broad_gains,
        jnp.cos(angles),
        jnp.sin(angles) * sign,
        mixer_gain[None, :],
        tokens,
        channel_gain[None, :],
        picker,
        route_columns,
        output_weight,
    )


def experts_kernel(
    width,
    out_going,
    gate_hbm,
    up_hbm,
    down_hbm,
    out_ref,
    rows,
    gate_w,
    up_w,
    down_w,
    hidden,
    gate_acc,
    up_acc,
    result,
    swap_send,
    swap_recv,
    back,
    w_sem,
    send_sem,
    recv_sem,
    h_send,
    h_recv,
    e_send,
    e_recv,
    b_send,
    b_recv,
):
    z, core, tp, sibling, x_peer, y_peer, chunks = place()
    chips, cap = out_going.shape[0], out_going.shape[1]
    ff = gate_acc.shape[1]
    half = 2 * cap
    ahead = [{"sp": ((z + d) % chips) * 2 + core, "tp": tp} for d in range(chips)]
    behind = [{"sp": ((z + chips - d) % chips) * 2 + core, "tp": tp} for d in range(chips)]
    enter(ahead[1:] + [sibling, x_peer, y_peer])

    def slot(d, r, side=0):
        return rows.at[d // 2, r, pl.ds(side * half + (d % 2) * cap, cap)]

    Z, X, Y, RELAY, SIDE = 0, 1, 2, 3, 4
    pending = []

    def send(source, target, kind, d, device):
        copy = remote(source, target, send_sem.at[kind, d], recv_sem.at[kind, d], device)
        copy.start()
        pending.append(copy)
        return copy

    arrivals = {}
    for d in range(1, chips):
        arrivals[Z, d] = send(out_going.at[d], slot(d, 0), Z, d, ahead[d])
    loads = [
        pltpu.make_async_copy(source, target, w_sem.at[i])
        for i, (source, target) in enumerate(
            ((gate_hbm, gate_w), (up_hbm, up_w), (down_hbm, down_w))
        )
    ]

    def spread(d):
        source = out_going.at[0] if d == 0 else slot(d, 0)
        if d:
            arrivals[Z, d].wait_recv()
        arrivals[X, d] = send(source, slot(d, 1), X, d, x_peer)
        arrivals[Y, d] = send(source, slot(d, 2), Y, d, y_peer)
        arrivals[SIDE, d] = send(source, slot(d, 0, 1), SIDE, d, sibling)

    def to_side(d, r):
        arrivals[SIDE + r, d] = send(slot(d, r), slot(d, r, 1), SIDE + r, d, sibling)

    def relay(d):
        arrivals[X, d].wait_recv()
        if d % 2 == 0:
            arrivals[RELAY, d] = send(slot(d, 1), slot(d, 3), RELAY, d, y_peer)
        to_side(d, 1)
        arrivals[Y, d].wait_recv()
        if d % 2 == 1:
            arrivals[RELAY, d] = send(slot(d, 2), slot(d, 3), RELAY, d, x_peer)
        to_side(d, 2)

    def project(p, r):
        for d in (2 * p, 2 * p + 1):
            arrivals[SIDE + r, d].wait_recv()
        block = rows[p, r, :, pl.ds(0, width)]
        for weight, total in ((gate_w, gate_acc), (up_w, up_acc)):
            part = jnp.dot(block, weight[chunks[r]], preferred_element_type=jnp.float32)
            if r == 0:
                total[...] = part
            else:
                total[...] += part

    def activate(p):
        squares = 0.0
        for r in range(4):
            extra = rows[p, r, :, pl.ds(width, EXTRA)].astype(jnp.float32)
            squares = squares + extra[:, 0:1] + extra[:, 1:2]
        scale = lax.rsqrt(squares / (4 * width) + epsilon)
        gate_value = gate_acc[...] * scale
        up_value = up_acc[...] * scale
        hidden[p, 0] = (gate_value / (1.0 + jnp.exp(-gate_value)) * up_value).astype(jnp.bfloat16)
        for k, peer in ((0, x_peer), (1, y_peer)):
            copy = remote(
                hidden.at[p, 0], hidden.at[p, 1 + k], h_send.at[p, k], h_recv.at[p, k], peer
            )
            copy.start()
            pending.append(copy)
            arrivals["h", p, k] = copy

    def relay_hidden(p):
        for k, peer in ((0, y_peer), (1, x_peer)):
            arrivals["h", p, k].wait_recv()
            part = pl.ds(k * half, half)
            copy = remote(
                hidden.at[p, 1 + k, part],
                hidden.at[p, 3, part],
                h_send.at[p, 2 + k],
                h_recv.at[p, 2 + k],
                peer,
            )
            copy.start()
            pending.append(copy)
            arrivals["h", p, 2 + k] = copy

    def last_slot(p):
        for d in (2 * p, 2 * p + 1):
            arrivals[RELAY, d].wait_recv()
            to_side(d, 3)
        project(p, 3)
        activate(p)

    def finish(p):
        for r in range(3):
            part = jnp.dot(hidden[p, r], down_w[chunks[r]], preferred_element_type=jnp.float32)
            if r == 0:
                result[...] = part
            else:
                result[...] += part
        for k in (2, 3):
            arrivals["h", p, k].wait_recv()
        result[...] += jnp.dot(hidden[p, 3], down_w[chunks[3]], preferred_element_type=jnp.float32)
        extra = rows[p, 0, :, pl.ds(width, EXTRA)].astype(jnp.float32)
        low = extra[:, 2:3] + extra[:, 3:4]
        high = extra[:, 4:5] + extra[:, 5:6]
        share = low + (high - low) * core.astype(jnp.float32)
        swap_send[p] = (result[half:, :] * share[half:]).astype(jnp.bfloat16)
        copy = remote(swap_send.at[p], swap_recv.at[p], e_send.at[p], e_recv.at[p], sibling)
        copy.start()
        pending.append(copy)
        kept = result[:half, :] * share[:half]
        copy.wait_recv()
        total = (kept + swap_recv[p].astype(jnp.float32)).astype(jnp.bfloat16)
        back[p] = total
        for d in (2 * p, 2 * p + 1):
            part = pl.ds((d % 2) * cap, cap)
            if d == 0:
                out_ref[0] = total[:cap]
                continue
            copy = remote(back.at[p, part], out_ref.at[d], b_send.at[d], b_recv.at[d], behind[d])
            copy.start()
            pending.append(copy)
            arrivals["b", d] = copy

    spread(0)
    for copy in loads:
        copy.start()
    rows[0, 0, pl.ds(0, cap)] = out_going[0]
    spread(1)
    relay(0)
    relay(1)
    spread(2)
    spread(3)
    loads[0].wait()
    loads[1].wait()
    for r in range(3):
        project(0, r)
    last_slot(0)
    relay(2)
    relay(3)
    relay_hidden(0)
    for r in range(3):
        project(1, r)
    last_slot(1)
    loads[2].wait()
    finish(0)
    relay_hidden(1)
    finish(1)
    for d in range(1, chips):
        arrivals["b", d].wait_recv()
    for copy in pending:
        copy.wait_send()


def run_experts(out_going, gate_weight, up_weight, down_weight):
    chips, cap, padded = out_going.shape
    width, ff = (padded - EXTRA, gate_weight.shape[1])
    features = down_weight.shape[1]
    return pl.pallas_call(
        functools.partial(experts_kernel, width),
        out_shape=jax.ShapeDtypeStruct((chips, cap, features), jnp.bfloat16),
        in_specs=[pl.BlockSpec(memory_space=pltpu.VMEM)]
        + [pl.BlockSpec(memory_space=pl.ANY)] * 3,
        out_specs=pl.BlockSpec(memory_space=pltpu.VMEM),
        scratch_shapes=[
            pltpu.VMEM((2, 4, 4 * cap, padded), jnp.bfloat16),
            pltpu.VMEM((4, width, ff), jnp.bfloat16),
            pltpu.VMEM((4, width, ff), jnp.bfloat16),
            pltpu.VMEM((4, ff, features), jnp.bfloat16),
            pltpu.VMEM((2, 4, 4 * cap, ff), jnp.bfloat16),
            pltpu.VMEM((4 * cap, ff), jnp.float32),
            pltpu.VMEM((4 * cap, ff), jnp.float32),
            pltpu.VMEM((4 * cap, features), jnp.float32),
            pltpu.VMEM((2, 2 * cap, features), jnp.bfloat16),
            pltpu.VMEM((2, 2 * cap, features), jnp.bfloat16),
            pltpu.VMEM((2, 2 * cap, features), jnp.bfloat16),
            pltpu.SemaphoreType.DMA((3,)),
            pltpu.SemaphoreType.DMA((8, 4)),
            pltpu.SemaphoreType.DMA((8, 4)),
            pltpu.SemaphoreType.DMA((2, 4)),
            pltpu.SemaphoreType.DMA((2, 4)),
            pltpu.SemaphoreType.DMA((2,)),
            pltpu.SemaphoreType.DMA((2,)),
            pltpu.SemaphoreType.DMA((4,)),
            pltpu.SemaphoreType.DMA((4,)),
        ],
        compiler_params=pltpu.CompilerParams(
            collective_id=2, has_side_effects=True, vmem_limit_bytes=56 * 1024 * 1024
        ),
    )(
        out_going,
        gate_weight.reshape(4, width, ff),
        up_weight.reshape(4, width, ff),
        down_weight.reshape(4, ff, features),
    )


def split_pair(values):
    high = lax.reduce_precision(values, 8, 7)
    return high, values - high


def paired_block(
    chips,
    positions,
    tokens,
    lean,
    lean_gains,
    broad,
    broad_gains,
    mixer_gain,
    output_weight,
    channel_gain,
    expert_weights,
    route_experts,
    weights,
):
    row_count, width = tokens.shape
    cap = row_count // 2
    group = route_experts[:, 0] // 2
    near = (group + GROUPS - lax.axis_index("sp") // 2) % GROUPS
    member = (near[:, None] == jnp.arange(GROUPS, dtype=jnp.int32)[None, :]).astype(jnp.bfloat16)
    order = jnp.arange(row_count, dtype=jnp.int32)
    earlier = (order[:, None] > order[None, :]).astype(jnp.bfloat16)
    counts = jnp.dot(earlier, member, preferred_element_type=jnp.float32)
    rank = jnp.sum(counts * member.astype(jnp.float32), axis=1).astype(jnp.int32)
    slot_index = near * cap + rank
    slots = jnp.arange(GROUPS * cap, dtype=jnp.int32)
    picker = (slots[:, None] == slot_index[None, :]).astype(jnp.bfloat16)
    first_low = route_experts[:, 0] % 2 == 0
    low = jnp.where(first_low, weights[:, 0], weights[:, 1])
    high = jnp.where(first_low, weights[:, 1], weights[:, 0])
    lane = jnp.arange(EXTRA, dtype=jnp.int32)[None, :]
    route_columns = jnp.zeros((row_count, EXTRA), jnp.float32)
    for i, column in enumerate(split_pair(low) + split_pair(high)):
        route_columns = jnp.where(lane == 2 + i, column[:, None], route_columns)
    stream, out_going = run_front(
        chips,
        positions,
        lean,
        broad,
        lean_gains,
        broad_gains,
        mixer_gain,
        tokens,
        channel_gain,
        picker,
        route_columns,
        output_weight,
    )
    arrived = run_experts(out_going.reshape(GROUPS, cap, width + EXTRA), *expert_weights)
    arrived = arrived.reshape(GROUPS * cap, width)
    picked = lax.dot_general(
        picker, arrived, (((0,), (0,)), ((), ())), preferred_element_type=jnp.float32
    )
    return (stream + picked).astype(jnp.bfloat16)


def on_device(
    tokens,
    lean_query,
    lean_key,
    lean_value,
    lean_gains,
    broad_query,
    broad_key,
    broad_value,
    broad_gains,
    mixer_gain,
    output_weight,
    channel_gain,
    gate_weight,
    up_weight,
    down_weight,
    route_experts,
    route_logits,
    group_weight,
):
    row_count = tokens.shape[0]
    positions = lax.axis_index("sp") * row_count + jnp.arange(row_count, dtype=jnp.int32)
    lane_index = lax.axis_index("tp")
    logit_gap = route_logits[:, 0] - route_logits[:, 1]
    weights = group_weight[:, None] * jax.nn.sigmoid(jnp.stack([logit_gap, -logit_gap], axis=1))
    chips = lax.axis_size("sp") // 2
    if (
        lax.axis_size("tp") == 4
        and chips == GROUPS
        and chips == 4
        and route_experts.shape[1] == 2
        and lean_query.shape[1:] == (4, 64)
        and broad_query.shape[1:] == (4, 128)
        and lean_key.shape[1:] == (2, 64)
        and broad_key.shape[1:] == (2, 128)
    ):
        return paired_block(
            chips,
            positions,
            tokens,
            (lean_query, lean_key, lean_value),
            lean_gains,
            (broad_query, broad_key, broad_value),
            broad_gains,
            mixer_gain,
            output_weight,
            channel_gain,
            (gate_weight[0], up_weight[0], down_weight[0]),
            route_experts,
            weights,
        )
    lean_queries, lean_keys, lean_values = own_heads(
        lean_query, lean_key, lean_value, lean_gains, positions, lane_index, HQ_A // KV_A
    )
    broad_queries, broad_keys, broad_values = own_heads(
        broad_query, broad_key, broad_value, broad_gains, positions, lane_index, HQ_B // KV_B
    )
    shard_rows = (
        lax.all_gather(lean_keys, "sp", axis=0, tiled=True),
        lax.all_gather(lean_values, "sp", axis=0, tiled=True),
        lax.all_gather(broad_keys, "sp", axis=0, tiled=True),
        lax.all_gather(broad_values, "sp", axis=0, tiled=True),
    )
    lean_state = attend_piece(start_state(lean_queries), lean_queries, shard_rows[0], shard_rows[1])
    broad_state = attend_piece(
        start_state(broad_queries), broad_queries, shard_rows[2], shard_rows[3]
    )
    lean_all, broad_all = (
        lax.all_gather(finish_heads(lean_state), "tp", axis=1, tiled=True),
        lax.all_gather(finish_heads(broad_state), "tp", axis=1, tiled=True),
    )
    lean_width = lean_all.shape[1]
    stream = tokens.astype(jnp.float32) + jnp.dot(
        group_norm(lean_all, mixer_gain[:lean_width]),
        output_weight[:lean_width],
        preferred_element_type=jnp.float32,
    )
    stream = stream + jnp.dot(
        group_norm(broad_all, mixer_gain[lean_width:]),
        output_weight[lean_width:],
        preferred_element_type=jnp.float32,
    )
    squares = lax.psum(jnp.sum(stream * stream, axis=1), "tp")
    normed = (stream * lax.rsqrt(squares / D + epsilon)[:, None] * channel_gain).astype(
        jnp.bfloat16
    )
    experts = lax.axis_size("sp")
    capacity = row_count // (experts // GROUPS)
    flat_experts = route_experts.reshape(-1)
    onehot = (flat_experts[:, None] == jnp.arange(experts, dtype=jnp.int32)[None, :]).astype(
        jnp.int32
    )
    slot_rank = jnp.sum((jnp.cumsum(onehot, axis=0) - 1) * onehot, axis=1)
    slot_index = flat_experts * capacity + slot_rank
    token_owner = jnp.repeat(jnp.arange(row_count, dtype=jnp.int32), route_experts.shape[1])
    filled = jnp.zeros((experts * capacity,), jnp.int32).at[slot_index].set(token_owner + 1)
    slot_live = (filled > 0)[:, None]
    source = jnp.maximum(filled - 1, 0)
    outgoing = jnp.where(slot_live, normed[source], jnp.zeros((), jnp.bfloat16)).reshape(
        experts, capacity, -1
    )
    arrived = lax.all_to_all(outgoing, "sp", split_axis=0, concat_axis=0, tiled=True)
    sources = arrived.shape[0]
    item_count = arrived.shape[1]
    shard_rows = lax.all_gather(arrived, "tp", axis=2, tiled=True)
    flat_rows = shard_rows.reshape(sources * item_count, shard_rows.shape[2])
    gate_part = gate_weight[0]
    up_part = up_weight[0]
    gate_value = jnp.dot(flat_rows, gate_part, preferred_element_type=jnp.float32)
    up_value = jnp.dot(flat_rows, up_part, preferred_element_type=jnp.float32)
    hidden = (jax.nn.silu(gate_value) * up_value).astype(jnp.bfloat16)
    down_part = down_weight[0]
    result = jnp.dot(
        lax.all_gather(hidden, "tp", axis=1, tiled=True),
        down_part,
        preferred_element_type=jnp.float32,
    )
    result = result.astype(jnp.bfloat16).reshape(sources, item_count, -1)
    returned = lax.all_to_all(result, "sp", split_axis=0, concat_axis=0, tiled=True)
    picked = (
        returned.reshape(experts * capacity, -1)[slot_index]
        .reshape(row_count, route_experts.shape[1], -1)
        .astype(jnp.float32)
    )
    return (stream + jnp.sum(picked * weights[:, :, None], axis=1)).astype(jnp.bfloat16)


def solution(mesh):
    return jax.shard_map(
        on_device,
        mesh=mesh,
        in_specs=(
            P("sp", "tp"),
            P("sp", "tp", None),
            P("sp", None, None),
            P("sp", None, None),
            P(),
            P("sp", "tp", None),
            P("sp", None, None),
            P("sp", None, None),
            P(),
            P(),
            P(None, "tp"),
            P("tp"),
            P("sp", None, "tp"),
            P("sp", None, "tp"),
            P("sp", None, "tp"),
            P("sp", None),
            P("sp", None),
            P("sp"),
        ),
        out_specs=P("sp", "tp"),
        check_vma=False,
    )
```

```python
import functools

import jax
import jax.numpy as jnp
import numpy as np
from jax import lax
from jax.experimental import pallas as pl
from jax.experimental.pallas import tpu as pltpu
from jax.sharding import PartitionSpec as P

D = 4096
HQ_A = 16
KV_A = 2
HQ_B = 16
KV_B = 2
GRID_W = 64
GROUPS = 4


epsilon = 1e-06
theta_base = 10000.0
floor_score = -1e30


def axial_angles(positions, head_size):
    quarter = head_size // 4
    frequency = theta_base ** (-jnp.arange(quarter, dtype=jnp.float32) / quarter)
    grid_rows = (positions // GRID_W).astype(jnp.float32)
    grid_columns = (positions % GRID_W).astype(jnp.float32)
    return (grid_rows[:, None] * frequency[None, :], grid_columns[:, None] * frequency[None, :])


def turn_half(values, angles):
    half_width = values.shape[-1] // 2
    first_half = values[..., :half_width]
    second = values[..., half_width:]
    cosine = jnp.cos(angles)[:, None, :]
    sine_part = jnp.sin(angles)[:, None, :]
    return jnp.concatenate(
        [first_half * cosine - second * sine_part, second * cosine + first_half * sine_part],
        axis=-1,
    )


def prepare(raw_values, gain_row, positions):
    values = raw_values.astype(jnp.float32)
    values = (
        values * lax.rsqrt(jnp.mean(values * values, axis=-1, keepdims=True) + epsilon) * gain_row
    )
    row_angles, column_angles = axial_angles(positions, raw_values.shape[-1])
    half_width = raw_values.shape[-1] // 2
    turned = jnp.concatenate(
        [
            turn_half(values[..., :half_width], row_angles),
            turn_half(values[..., half_width:], column_angles),
        ],
        axis=-1,
    )
    return turned.astype(jnp.bfloat16)


def group_norm(head_rows, gain_row):
    values = head_rows.astype(jnp.float32)
    return (
        values * lax.rsqrt(jnp.mean(values * values, axis=-1, keepdims=True) + epsilon) * gain_row
    ).astype(jnp.bfloat16)


def own_heads(query_raw, key_raw, value_raw, gain_pair, positions, lane_index, group_ratio):
    head_count, head_size = (query_raw.shape[1], query_raw.shape[2])
    key_heads = max(1, head_count // group_ratio)
    kv_start = lane_index * head_count // group_ratio
    key_part = lax.dynamic_slice_in_dim(key_raw, kv_start, key_heads, 1)
    value_part = lax.dynamic_slice_in_dim(value_raw, kv_start, key_heads, 1)
    queries = prepare(query_raw, gain_pair[0], positions).reshape(
        query_raw.shape[0], key_heads, head_count // key_heads, head_size
    )
    return (queries, prepare(key_part, gain_pair[1], positions), value_part)


def start_state(queries):
    row_count = queries.shape[0]
    head_count = queries.shape[1] * queries.shape[2]
    return (
        jnp.full((head_count, row_count), floor_score, jnp.float32),
        jnp.zeros((head_count, row_count), jnp.float32),
        jnp.zeros((row_count, head_count, queries.shape[3]), jnp.float32),
    )


def attend_piece(fold_state, queries, keys, values):
    peak_score, weight_sum, accumulated = fold_state
    row_count, key_heads, grouped, head_size = queries.shape
    key_count = keys.shape[0]
    scores = jnp.einsum(
        "qkgd,skd->kgqs", queries, keys, preferred_element_type=jnp.float32
    ) * head_size ** (-0.5)
    scores = scores.reshape(key_heads * grouped, row_count, key_count)
    new_peak = jnp.maximum(peak_score, jnp.max(scores, axis=-1))
    weights = jnp.exp(scores - new_peak[..., None])
    new_sum = jnp.sum(weights, axis=-1)
    rounded = weights.astype(jnp.bfloat16).reshape(key_heads, grouped, row_count, key_count)
    partial_value = jnp.einsum(
        "kgqs,skd->qkgd", rounded, values, preferred_element_type=jnp.float32
    )
    partial_value = partial_value.reshape(row_count, key_heads * grouped, head_size)
    return (new_peak, new_sum, partial_value)


def finish_heads(fold_state):
    accumulated = fold_state[2]
    return (
        (accumulated / jnp.transpose(fold_state[1])[:, :, None])
        .astype(jnp.bfloat16)
        .reshape(accumulated.shape[0], -1)
    )


MESH = pl.DeviceIdType.MESH
EXTRA = 128


def enter(peers):
    barrier = pltpu.get_barrier_semaphore()
    for peer in peers:
        pl.semaphore_signal(barrier, inc=1, device_id=peer, device_id_type=MESH)
    pl.semaphore_wait(barrier, len(peers))


def place():
    sp, tp = lax.axis_index("sp"), lax.axis_index("tp")
    z, core = sp // 2, sp % 2
    y, x = tp // 2, tp % 2
    sibling = {"sp": z * 2 + (1 - core), "tp": tp}
    x_peer = {"sp": sp, "tp": y * 2 + (1 - x)}
    y_peer = {"sp": sp, "tp": (1 - y) * 2 + x}
    chunks = (tp, y * 2 + (1 - x), (1 - y) * 2 + x, (1 - y) * 2 + (1 - x))
    return z, core, tp, sibling, x_peer, y_peer, chunks


def remote(source, target, send_sem, recv_sem, device):
    return pltpu.make_async_remote_copy(
        src_ref=source,
        dst_ref=target,
        send_sem=send_sem,
        recv_sem=recv_sem,
        device_id=device,
        device_id_type=MESH,
    )


def front_kernel(
    chips,
    lean_q,
    lean_k,
    lean_v,
    broad_q,
    broad_k,
    broad_v,
    lean_gain,
    broad_gain,
    cosines,
    sines,
    mixer_gain,
    tokens,
    channel_gain,
    picker,
    route_columns,
    weight_hbm,
    stream_out,
    going_out,
    own,
    keys,
    queries,
    peak,
    total,
    mass,
    lean_heads,
    broad_heads,
    weight,
    lean_acc,
    broad_acc,
    w_sem,
    k_send,
    k_recv,
    h_send,
    h_recv,
):
    z, core, tp, sibling, x_peer, y_peer, chunks = place()
    x, y = tp % 2, tp // 2
    rows = own.shape[0]
    half = rows // 2
    lanes = 128
    peers = [{"sp": ((z + d) % chips) * 2 + core, "tp": tp} for d in range(1, chips)]
    load = pltpu.make_async_copy(weight_hbm, weight, w_sem.at[0])
    load.start()
    lane = lax.broadcasted_iota(jnp.int32, (rows, lanes), 1)
    low = lane < lanes // 2

    def turned(raw, gain, size):
        values = raw.astype(jnp.float32)
        squares = values * values
        if size == lanes:
            mean = jnp.sum(squares, axis=1, keepdims=True) / size
        else:
            first = jnp.sum(jnp.where(low, squares, 0.0), axis=1, keepdims=True)
            second = jnp.sum(jnp.where(low, 0.0, squares), axis=1, keepdims=True)
            mean = jnp.where(low, first, second) / size
        values = values * lax.rsqrt(mean + epsilon) * gain
        quarter = size // 4
        partner = jnp.where(
            lane % (2 * quarter) < quarter,
            pltpu.roll(values, lanes - quarter, 1),
            pltpu.roll(values, quarter, 1),
        )
        part = pl.ds(0 if size == lanes else lanes, lanes)
        return values * cosines[:, part] + partner * sines[:, part]

    def swapped(values):
        return pltpu.roll(values, lanes // 2, 1)

    key_columns = pl.ds(pl.multiple_of(y * lanes, lanes), lanes)
    own[:, :lanes] = turned(broad_k[:, key_columns], broad_gain[1:2, :], lanes).astype(jnp.bfloat16)
    own[:, lanes : 2 * lanes] = broad_v[:, key_columns]
    both_keys = turned(lean_k[...], lean_gain[1:2, :], lanes // 2)
    both_values = lean_v[...].astype(jnp.float32)
    at_first = (1 - y).astype(jnp.float32)
    lean_key = both_keys * at_first + swapped(both_keys) * (1.0 - at_first)
    lean_value = swapped(both_values) * at_first + both_values * (1.0 - at_first)
    own[:, 2 * lanes :] = jnp.where(low, lean_key, lean_value).astype(jnp.bfloat16)

    enter(peers + [sibling, x_peer, y_peer])
    pending = []
    arrivals = {}

    def send(kind, d, source, target, device):
        copy = remote(source, target, k_send.at[kind, d], k_recv.at[kind, d], device)
        copy.start()
        pending.append(copy)
        arrivals[kind, d] = copy

    mine = pl.ds(pl.multiple_of(x * half, half), half)
    other = pl.ds(pl.multiple_of((1 - x) * half, half), half)
    side_mine = pl.ds(pl.multiple_of(rows + x * half, half), half)
    side_other = pl.ds(pl.multiple_of(rows + (1 - x) * half, half), half)
    Z, X, A, B = 0, 1, 2, 3
    for d in range(1, chips):
        send(Z, d, own.at[mine], keys.at[d, mine], peers[d - 1])
    send(A, 0, own, keys.at[0, pl.ds(rows, rows)], sibling)
    keys[0, pl.ds(0, rows)] = own[...]

    heads = queries.shape[1]
    for h in range(heads):
        part = pl.ds(h * lanes, lanes)
        queries[1, h] = turned(broad_q[:, part], broad_gain[0:1, :], lanes).astype(jnp.bfloat16)
    for h in range(heads // 2):
        part = pl.ds(h * lanes, lanes)
        pair = turned(lean_q[:, part], lean_gain[0:1, :], lanes // 2)
        queries[0, 2 * h] = jnp.where(low, pair, 0.0).astype(jnp.bfloat16)
        queries[0, 2 * h + 1] = jnp.where(low, swapped(pair), 0.0).astype(jnp.bfloat16)

    def attend(d, kind):
        size = lanes // 2 if kind == 0 else lanes
        key_part = pl.ds(2 * lanes, lanes) if kind == 0 else pl.ds(0, lanes)
        value_part = pl.ds(2 * lanes, lanes) if kind == 0 else pl.ds(lanes, lanes)

        def one_head(h, carry):
            scores = lax.dot_general(
                queries[kind, h],
                keys[d, :, key_part],
                (((1,), (1,)), ((), ())),
                preferred_element_type=jnp.float32,
            ) * (size**-0.5)
            top = jnp.max(scores, axis=1, keepdims=True)
            if d:
                old = peak[kind, h][:, :1]
                top = jnp.maximum(old, top)
            weights = jnp.exp(scores - top)
            summed = jnp.sum(weights, axis=1, keepdims=True)
            partial = jnp.dot(
                weights.astype(jnp.bfloat16),
                keys[d, :, value_part],
                preferred_element_type=jnp.float32,
            )
            if d:
                shrink = jnp.exp(old - top)
                summed = summed + total[kind, h][:, :1] * shrink
                partial = partial + mass[kind, h] * shrink
            peak[kind, h] = jnp.broadcast_to(top, (rows, lanes))
            total[kind, h] = jnp.broadcast_to(summed, (rows, lanes))
            mass[kind, h] = partial
            return carry

        lax.fori_loop(0, heads, one_head, 0)

    def forward(d):
        arrivals[Z, d].wait_recv()
        send(X, d, keys.at[d, mine], keys.at[d, mine], x_peer)
        send(A, d, keys.at[d, mine], keys.at[d, side_mine], sibling)

    def forward_other(d):
        arrivals[X, d].wait_recv()
        send(B, d, keys.at[d, other], keys.at[d, side_other], sibling)

    forward(1)
    arrivals[A, 0].wait_recv()
    attend(0, 0)
    forward_other(1)
    attend(0, 1)
    for d in range(1, chips):
        if d + 1 < chips:
            forward(d + 1)
        arrivals[A, d].wait_recv()
        arrivals[B, d].wait_recv()
        if d + 1 < chips:
            attend(d, 0)
            forward_other(d + 1)
            attend(d, 1)

    gathers = {}

    def spread(kind, buffer):
        for k, peer in ((0, x_peer), (1, y_peer)):
            n = kind * 4 + k
            copy = remote(buffer.at[0], buffer.at[1 + k], h_send.at[n], h_recv.at[n], peer)
            copy.start()
            pending.append(copy)
            gathers[kind, k] = copy

    def relay(kind, buffer):
        for k, peer in ((0, y_peer), (1, x_peer)):
            n = kind * 4 + 2 + k
            gathers[kind, k].wait_recv()
            part = pl.ds(k * half, half)
            copy = remote(
                buffer.at[1 + k, part], buffer.at[3, part], h_send.at[n], h_recv.at[n], peer
            )
            copy.start()
            pending.append(copy)
            gathers[kind, 2 + k] = copy

    def finished(kind, h):
        return mass[kind, h] / total[kind, h]

    attend(chips - 1, 0)
    for h in range(heads // 2):
        pair = jnp.where(low, swapped(finished(0, 2 * h)), finished(0, 2 * h + 1))
        lean_heads[0, :, pl.ds(h * lanes, lanes)] = pair.astype(jnp.bfloat16)
    spread(0, lean_heads)
    attend(chips - 1, 1)
    for h in range(heads):
        broad_heads[0, :, pl.ds(h * lanes, lanes)] = finished(1, h).astype(jnp.bfloat16)
    spread(1, broad_heads)
    load.wait()
    lean_width, broad_width = lean_heads.shape[2], broad_heads.shape[2]
    squares = [0.0, 0.0]

    def project(kind, r):
        buffer, acc, width, start = (
            (lean_heads, lean_acc, lean_width, 0),
            (broad_heads, broad_acc, broad_width, 4 * lean_width),
        )[kind]
        part = pl.ds(pl.multiple_of(start + chunks[r] * width, width), width)
        values = buffer[r].astype(jnp.float32)
        squares[kind] = squares[kind] + jnp.sum(values * values, axis=1, keepdims=True)
        scaled = (values * mixer_gain[:, part]).astype(jnp.bfloat16)
        product = jnp.dot(scaled, weight[part, :], preferred_element_type=jnp.float32)
        if r == 0:
            acc[...] = product
        else:
            acc[...] += product

    project(0, 0)
    relay(0, lean_heads)
    project(1, 0)
    project(0, 1)
    project(0, 2)
    relay(1, broad_heads)
    project(1, 1)
    project(1, 2)
    for kind in (0, 1):
        gathers[kind, 2].wait_recv()
        gathers[kind, 3].wait_recv()
        project(kind, 3)
    lean_scale = lax.rsqrt(squares[0] / (4 * lean_width) + epsilon)
    broad_scale = lax.rsqrt(squares[1] / (4 * broad_width) + epsilon)
    stream = (
        tokens[...].astype(jnp.float32)
        + lean_acc[...] * lean_scale
        + broad_acc[...] * broad_scale
    )
    stream_out[...] = stream
    width = stream.shape[1]
    norm = jnp.sum(stream * stream, axis=1, keepdims=True)
    norm_high = norm.astype(jnp.bfloat16).astype(jnp.float32)
    extra = jnp.where(
        lane == 0, norm_high, jnp.where(lane == 1, norm - norm_high, route_columns[...])
    ).astype(jnp.bfloat16)
    scaled = (stream * channel_gain[...]).astype(jnp.bfloat16)
    going_out[:, :width] = jnp.dot(
        picker[...], scaled, preferred_element_type=jnp.float32
    ).astype(jnp.bfloat16)
    going_out[:, width:] = jnp.dot(
        picker[...], extra, preferred_element_type=jnp.float32
    ).astype(jnp.bfloat16)
    for copy in pending:
        copy.wait_send()


def lane_frequencies(head_size):
    quarter = head_size // 4
    lane = np.arange(128) % head_size
    frequency = theta_base ** (-(lane % quarter).astype(np.float32) / np.float32(quarter))
    by_row = lane < head_size // 2
    sign = np.where(lane // quarter % 2 == 0, -1.0, 1.0)
    return frequency.astype(np.float32), by_row, sign.astype(np.float32)


def run_front(
    chips,
    positions,
    lean,
    broad,
    lean_gains,
    broad_gains,
    mixer_gain,
    tokens,
    channel_gain,
    picker,
    route_columns,
    output_weight,
):
    rows, width = tokens.shape
    heads = lean[0].shape[1]
    tables = [lane_frequencies(part[0].shape[2]) for part in (broad, lean)]
    frequency, by_row, sign = (np.concatenate(parts)[None, :] for parts in zip(*tables))
    row = (positions // GRID_W).astype(jnp.float32)[:, None]
    column = (positions % GRID_W).astype(jnp.float32)[:, None]
    angles = jnp.where(by_row, row, column) * frequency
    flat = [part.reshape(rows, -1) for part in lean + broad]
    return pl.pallas_call(
        functools.partial(front_kernel, chips),
        out_shape=[
            jax.ShapeDtypeStruct((rows, width), jnp.float32),
            jax.ShapeDtypeStruct((picker.shape[0], width + EXTRA), jnp.bfloat16),
        ],
        in_specs=[pl.BlockSpec(memory_space=pltpu.VMEM)] * 15
        + [pl.BlockSpec(memory_space=pl.ANY)],
        out_specs=[pl.BlockSpec(memory_space=pltpu.VMEM)] * 2,
        scratch_shapes=[
            pltpu.VMEM((rows, 384), jnp.bfloat16),
            pltpu.VMEM((chips, 2 * rows, 384), jnp.bfloat16),
            pltpu.VMEM((2, heads, rows, 128), jnp.bfloat16),
            pltpu.VMEM((2, heads, rows, 128), jnp.float32),
            pltpu.VMEM((2, heads, rows, 128), jnp.float32),
            pltpu.VMEM((2, heads, rows, 128), jnp.float32),
            pltpu.VMEM((4, rows, heads * 64), jnp.bfloat16),
            pltpu.VMEM((4, rows, heads * 128), jnp.bfloat16),
            pltpu.VMEM(output_weight.shape, jnp.bfloat16),
            pltpu.VMEM((rows, width), jnp.float32),
            pltpu.VMEM((rows, width), jnp.float32),
            pltpu.SemaphoreType.DMA((1,)),
            pltpu.SemaphoreType.DMA((4, chips)),
            pltpu.SemaphoreType.DMA((4, chips)),
            pltpu.SemaphoreType.DMA((8,)),
            pltpu.SemaphoreType.DMA((8,)),
        ],
        compiler_params=pltpu.CompilerParams(
            collective_id=0, has_side_effects=True, vmem_limit_bytes=48 * 1024 * 1024
        ),
    )(
        *flat,
        jnp.concatenate([lean_gains, lean_gains], axis=1),
        broad_gains,
        jnp.cos(angles),
        jnp.sin(angles) * sign,
        mixer_gain[None, :],
        tokens,
        channel_gain[None, :],
        picker,
        route_columns,
        output_weight,
    )


def experts_kernel(
    width,
    out_going,
    gate_hbm,
    up_hbm,
    down_hbm,
    out_ref,
    rows,
    gate_w,
    up_w,
    down_w,
    hidden,
    gate_acc,
    up_acc,
    result,
    swap_send,
    swap_recv,
    back,
    w_sem,
    send_sem,
    recv_sem,
    h_send,
    h_recv,
    e_send,
    e_recv,
    b_send,
    b_recv,
):
    z, core, tp, sibling, x_peer, y_peer, chunks = place()
    chips, cap = out_going.shape[0], out_going.shape[1]
    part = cap // 2
    ahead = [{"sp": ((z + d) % chips) * 2 + core, "tp": tp} for d in range(chips)]
    behind = [{"sp": ((z + chips - d) % chips) * 2 + core, "tp": tp} for d in range(chips)]
    enter(ahead[1:] + [sibling, x_peer, y_peer])

    def slot(d, r, side=0):
        return rows.at[d, r, pl.ds(side * cap, cap)]

    Z, X, Y, VIA_X, VIA_Y, SIDE = 0, 1, 2, 3, 4, 5
    pending = []
    arrivals = {}

    def send(source, target, kind, d, device):
        copy = remote(source, target, send_sem.at[kind, d], recv_sem.at[kind, d], device)
        copy.start()
        pending.append(copy)
        arrivals[kind, d] = copy

    for d in range(1, chips):
        send(out_going.at[d], slot(d, 0), Z, d, ahead[d])
    loads = [
        pltpu.make_async_copy(source, target, w_sem.at[i])
        for i, (source, target) in enumerate(
            ((gate_hbm, gate_w), (up_hbm, up_w), (down_hbm, down_w))
        )
    ]

    def to_side(d, r):
        source = out_going.at[0] if d == 0 and r == 0 else slot(d, r)
        send(source, slot(d, r, 1), SIDE + r, d, sibling)

    def spread(d):
        source = out_going.at[0] if d == 0 else slot(d, 0)
        if d:
            arrivals[Z, d].wait_recv()
        send(source, slot(d, 1), X, d, x_peer)
        send(source, slot(d, 2), Y, d, y_peer)
        to_side(d, 0)

    def relay(d):
        for kind, r, peer in ((X, 1, y_peer), (Y, 2, x_peer)):
            arrivals[kind, d].wait_recv()
            piece = pl.ds((r - 1) * part, part)
            send(rows.at[d, r, piece], rows.at[d, 3, piece], VIA_X + r - 1, d, peer)
            to_side(d, r)

    def project(d):
        for r in range(4):
            if r == 3:
                arrivals[VIA_X, d].wait_recv()
                arrivals[VIA_Y, d].wait_recv()
                to_side(d, 3)
            arrivals[SIDE + r, d].wait_recv()
            block = rows[d, r, :, pl.ds(0, width)]
            for weight, total in ((gate_w, gate_acc), (up_w, up_acc)):
                product = jnp.dot(block, weight[chunks[r]], preferred_element_type=jnp.float32)
                if r == 0:
                    total[...] = product
                else:
                    total[...] += product
        squares = 0.0
        for r in range(4):
            extra = rows[d, r, :, pl.ds(width, EXTRA)].astype(jnp.float32)
            squares = squares + extra[:, 0:1] + extra[:, 1:2]
        scale = lax.rsqrt(squares / (4 * width) + epsilon)
        gate_value = gate_acc[...] * scale
        up_value = up_acc[...] * scale
        hidden[d, 0] = (gate_value / (1.0 + jnp.exp(-gate_value)) * up_value).astype(jnp.bfloat16)

    def send_hidden_piece(d, k, source, target, peer):
        copy = remote(source, target, h_send.at[d, k], h_recv.at[d, k], peer)
        copy.start()
        pending.append(copy)
        arrivals["h", d, k] = copy

    def spread_hidden(d):
        send_hidden_piece(d, 0, hidden.at[d, 0], hidden.at[d, 1], x_peer)
        send_hidden_piece(d, 1, hidden.at[d, 0], hidden.at[d, 2], y_peer)

    def relay_hidden(d):
        for k, peer in ((0, y_peer), (1, x_peer)):
            arrivals["h", d, k].wait_recv()
            piece = pl.ds(k * cap, cap)
            send_hidden_piece(d, 2 + k, hidden.at[d, 1 + k, piece], hidden.at[d, 3, piece], peer)

    def finish(d):
        for r in range(4):
            if r == 3:
                arrivals["h", d, 2].wait_recv()
                arrivals["h", d, 3].wait_recv()
            product = jnp.dot(hidden[d, r], down_w[chunks[r]], preferred_element_type=jnp.float32)
            if r == 0:
                result[...] = product
            else:
                result[...] += product
        extra = rows[d, 0, :, pl.ds(width, EXTRA)].astype(jnp.float32)
        low = extra[:, 2:3] + extra[:, 3:4]
        high = extra[:, 4:5] + extra[:, 5:6]
        share = low + (high - low) * core.astype(jnp.float32)
        swap_send[d] = (result[cap:, :] * share[cap:]).astype(jnp.bfloat16)
        copy = remote(swap_send.at[d], swap_recv.at[d], e_send.at[d], e_recv.at[d], sibling)
        copy.start()
        pending.append(copy)
        kept = result[:cap, :] * share[:cap]
        copy.wait_recv()
        total = (kept + swap_recv[d].astype(jnp.float32)).astype(jnp.bfloat16)
        if d == 0:
            out_ref[0] = total
            return
        back[d] = total
        copy = remote(back.at[d], out_ref.at[d], b_send.at[d], b_recv.at[d], behind[d])
        copy.start()
        pending.append(copy)
        arrivals["b", d] = copy

    spread(0)
    for copy in loads:
        copy.start()
    rows[0, 0, pl.ds(0, cap)] = out_going[0]
    relay(0)
    spread(1)
    relay(1)
    loads[0].wait()
    loads[1].wait()
    project(0)
    spread(2)
    project(1)
    spread_hidden(1)
    relay(2)
    spread(3)
    relay_hidden(1)
    project(2)
    spread_hidden(2)
    relay(3)
    loads[2].wait()
    finish(1)
    spread_hidden(0)
    relay_hidden(2)
    project(3)
    spread_hidden(3)
    finish(2)
    relay_hidden(0)
    relay_hidden(3)
    finish(3)
    finish(0)
    for d in range(1, chips):
        arrivals["b", d].wait_recv()
    for copy in pending:
        copy.wait_send()


def run_experts(out_going, gate_weight, up_weight, down_weight):
    chips, cap, padded = out_going.shape
    width, ff = (padded - EXTRA, gate_weight.shape[1])
    features = down_weight.shape[1]
    return pl.pallas_call(
        functools.partial(experts_kernel, width),
        out_shape=jax.ShapeDtypeStruct((chips, cap, features), jnp.bfloat16),
        in_specs=[pl.BlockSpec(memory_space=pltpu.VMEM)]
        + [pl.BlockSpec(memory_space=pl.ANY)] * 3,
        out_specs=pl.BlockSpec(memory_space=pltpu.VMEM),
        scratch_shapes=[
            pltpu.VMEM((chips, 4, 2 * cap, padded), jnp.bfloat16),
            pltpu.VMEM((4, width, ff), jnp.bfloat16),
            pltpu.VMEM((4, width, ff), jnp.bfloat16),
            pltpu.VMEM((4, ff, features), jnp.bfloat16),
            pltpu.VMEM((chips, 4, 2 * cap, ff), jnp.bfloat16),
            pltpu.VMEM((2 * cap, ff), jnp.float32),
            pltpu.VMEM((2 * cap, ff), jnp.float32),
            pltpu.VMEM((2 * cap, features), jnp.float32),
            pltpu.VMEM((chips, cap, features), jnp.bfloat16),
            pltpu.VMEM((chips, cap, features), jnp.bfloat16),
            pltpu.VMEM((chips, cap, features), jnp.bfloat16),
            pltpu.SemaphoreType.DMA((3,)),
            pltpu.SemaphoreType.DMA((9, chips)),
            pltpu.SemaphoreType.DMA((9, chips)),
            pltpu.SemaphoreType.DMA((chips, 4)),
            pltpu.SemaphoreType.DMA((chips, 4)),
            pltpu.SemaphoreType.DMA((chips,)),
            pltpu.SemaphoreType.DMA((chips,)),
            pltpu.SemaphoreType.DMA((chips,)),
            pltpu.SemaphoreType.DMA((chips,)),
        ],
        compiler_params=pltpu.CompilerParams(
            collective_id=2, has_side_effects=True, vmem_limit_bytes=56 * 1024 * 1024
        ),
    )(
        out_going,
        gate_weight.reshape(4, width, ff),
        up_weight.reshape(4, width, ff),
        down_weight.reshape(4, ff, features),
    )


def split_pair(values):
    high = lax.reduce_precision(values, 8, 7)
    return high, values - high


def paired_block(
    chips,
    positions,
    tokens,
    lean,
    lean_gains,
    broad,
    broad_gains,
    mixer_gain,
    output_weight,
    channel_gain,
    expert_weights,
    route_experts,
    weights,
):
    row_count, width = tokens.shape
    cap = row_count // 2
    group = route_experts[:, 0] // 2
    near = (group + GROUPS - lax.axis_index("sp") // 2) % GROUPS
    member = (near[:, None] == jnp.arange(GROUPS, dtype=jnp.int32)[None, :]).astype(jnp.bfloat16)
    order = jnp.arange(row_count, dtype=jnp.int32)
    earlier = (order[:, None] > order[None, :]).astype(jnp.bfloat16)
    counts = jnp.dot(earlier, member, preferred_element_type=jnp.float32)
    rank = jnp.sum(counts * member.astype(jnp.float32), axis=1).astype(jnp.int32)
    slot_index = near * cap + rank
    slots = jnp.arange(GROUPS * cap, dtype=jnp.int32)
    picker = (slots[:, None] == slot_index[None, :]).astype(jnp.bfloat16)
    first_low = route_experts[:, 0] % 2 == 0
    low = jnp.where(first_low, weights[:, 0], weights[:, 1])
    high = jnp.where(first_low, weights[:, 1], weights[:, 0])
    lane = jnp.arange(EXTRA, dtype=jnp.int32)[None, :]
    route_columns = jnp.zeros((row_count, EXTRA), jnp.float32)
    for i, column in enumerate(split_pair(low) + split_pair(high)):
        route_columns = jnp.where(lane == 2 + i, column[:, None], route_columns)
    stream, out_going = run_front(
        chips,
        positions,
        lean,
        broad,
        lean_gains,
        broad_gains,
        mixer_gain,
        tokens,
        channel_gain,
        picker,
        route_columns,
        output_weight,
    )
    arrived = run_experts(out_going.reshape(GROUPS, cap, width + EXTRA), *expert_weights)
    arrived = arrived.reshape(GROUPS * cap, width)
    picked = lax.dot_general(
        picker, arrived, (((0,), (0,)), ((), ())), preferred_element_type=jnp.float32
    )
    return (stream + picked).astype(jnp.bfloat16)


def on_device(
    tokens,
    lean_query,
    lean_key,
    lean_value,
    lean_gains,
    broad_query,
    broad_key,
    broad_value,
    broad_gains,
    mixer_gain,
    output_weight,
    channel_gain,
    gate_weight,
    up_weight,
    down_weight,
    route_experts,
    route_logits,
    group_weight,
):
    row_count = tokens.shape[0]
    positions = lax.axis_index("sp") * row_count + jnp.arange(row_count, dtype=jnp.int32)
    lane_index = lax.axis_index("tp")
    logit_gap = route_logits[:, 0] - route_logits[:, 1]
    weights = group_weight[:, None] * jax.nn.sigmoid(jnp.stack([logit_gap, -logit_gap], axis=1))
    chips = lax.axis_size("sp") // 2
    if (
        lax.axis_size("tp") == 4
        and chips == GROUPS
        and chips == 4
        and route_experts.shape[1] == 2
        and lean_query.shape[1:] == (4, 64)
        and broad_query.shape[1:] == (4, 128)
        and lean_key.shape[1:] == (2, 64)
        and broad_key.shape[1:] == (2, 128)
    ):
        return paired_block(
            chips,
            positions,
            tokens,
            (lean_query, lean_key, lean_value),
            lean_gains,
            (broad_query, broad_key, broad_value),
            broad_gains,
            mixer_gain,
            output_weight,
            channel_gain,
            (gate_weight[0], up_weight[0], down_weight[0]),
            route_experts,
            weights,
        )
    lean_queries, lean_keys, lean_values = own_heads(
        lean_query, lean_key, lean_value, lean_gains, positions, lane_index, HQ_A // KV_A
    )
    broad_queries, broad_keys, broad_values = own_heads(
        broad_query, broad_key, broad_value, broad_gains, positions, lane_index, HQ_B // KV_B
    )
    shard_rows = (
        lax.all_gather(lean_keys, "sp", axis=0, tiled=True),
        lax.all_gather(lean_values, "sp", axis=0, tiled=True),
        lax.all_gather(broad_keys, "sp", axis=0, tiled=True),
        lax.all_gather(broad_values, "sp", axis=0, tiled=True),
    )
    lean_state = attend_piece(start_state(lean_queries), lean_queries, shard_rows[0], shard_rows[1])
    broad_state = attend_piece(
        start_state(broad_queries), broad_queries, shard_rows[2], shard_rows[3]
    )
    lean_all, broad_all = (
        lax.all_gather(finish_heads(lean_state), "tp", axis=1, tiled=True),
        lax.all_gather(finish_heads(broad_state), "tp", axis=1, tiled=True),
    )
    lean_width = lean_all.shape[1]
    stream = tokens.astype(jnp.float32) + jnp.dot(
        group_norm(lean_all, mixer_gain[:lean_width]),
        output_weight[:lean_width],
        preferred_element_type=jnp.float32,
    )
    stream = stream + jnp.dot(
        group_norm(broad_all, mixer_gain[lean_width:]),
        output_weight[lean_width:],
        preferred_element_type=jnp.float32,
    )
    squares = lax.psum(jnp.sum(stream * stream, axis=1), "tp")
    normed = (stream * lax.rsqrt(squares / D + epsilon)[:, None] * channel_gain).astype(
        jnp.bfloat16
    )
    experts = lax.axis_size("sp")
    capacity = row_count // (experts // GROUPS)
    flat_experts = route_experts.reshape(-1)
    onehot = (flat_experts[:, None] == jnp.arange(experts, dtype=jnp.int32)[None, :]).astype(
        jnp.int32
    )
    slot_rank = jnp.sum((jnp.cumsum(onehot, axis=0) - 1) * onehot, axis=1)
    slot_index = flat_experts * capacity + slot_rank
    token_owner = jnp.repeat(jnp.arange(row_count, dtype=jnp.int32), route_experts.shape[1])
    filled = jnp.zeros((experts * capacity,), jnp.int32).at[slot_index].set(token_owner + 1)
    slot_live = (filled > 0)[:, None]
    source = jnp.maximum(filled - 1, 0)
    outgoing = jnp.where(slot_live, normed[source], jnp.zeros((), jnp.bfloat16)).reshape(
        experts, capacity, -1
    )
    arrived = lax.all_to_all(outgoing, "sp", split_axis=0, concat_axis=0, tiled=True)
    sources = arrived.shape[0]
    item_count = arrived.shape[1]
    shard_rows = lax.all_gather(arrived, "tp", axis=2, tiled=True)
    flat_rows = shard_rows.reshape(sources * item_count, shard_rows.shape[2])
    gate_part = gate_weight[0]
    up_part = up_weight[0]
    gate_value = jnp.dot(flat_rows, gate_part, preferred_element_type=jnp.float32)
    up_value = jnp.dot(flat_rows, up_part, preferred_element_type=jnp.float32)
    hidden = (jax.nn.silu(gate_value) * up_value).astype(jnp.bfloat16)
    down_part = down_weight[0]
    result = jnp.dot(
        lax.all_gather(hidden, "tp", axis=1, tiled=True),
        down_part,
        preferred_element_type=jnp.float32,
    )
    result = result.astype(jnp.bfloat16).reshape(sources, item_count, -1)
    returned = lax.all_to_all(result, "sp", split_axis=0, concat_axis=0, tiled=True)
    picked = (
        returned.reshape(experts * capacity, -1)[slot_index]
        .reshape(row_count, route_experts.shape[1], -1)
        .astype(jnp.float32)
    )
    return (stream + jnp.sum(picked * weights[:, :, None], axis=1)).astype(jnp.bfloat16)


def solution(mesh):
    return jax.shard_map(
        on_device,
        mesh=mesh,
        in_specs=(
            P("sp", "tp"),
            P("sp", "tp", None),
            P("sp", None, None),
            P("sp", None, None),
            P(),
            P("sp", "tp", None),
            P("sp", None, None),
            P("sp", None, None),
            P(),
            P(),
            P(None, "tp"),
            P("tp"),
            P("sp", None, "tp"),
            P("sp", None, "tp"),
            P("sp", None, "tp"),
            P("sp", None),
            P("sp", None),
            P("sp"),
        ),
        out_specs=P("sp", "tp"),
        check_vma=False,
    )
```
